32 devices in a mesh: rep: 2 (over x), fs: 8 (over z, y), tp: 2 (over core).
Axes of the slice: x: 2, y: 2, z: 4, core: 2. Of those that a mesh axis runs over, the one named last changes fastest.
Arguments:
- tokens: bfloat16 [16, 512, 2048], P(('rep', 'fs')), may hold values from -6 to 6
- gain_mix_pre: float32 [2048], P('fs'), may hold values from 0.1 to 1.9
- gain_mix_post: float32 [2048], P('fs'), may hold values from 0.1 to 1.9
- gain_mlp_pre: float32 [2048], P('fs'), may hold values from 0.1 to 1.9
- gain_mlp_post: float32 [2048], P('fs'), may hold values from 0.1 to 1.9
- x_weight: float32 [2048, 2048], P('fs', 'tp'), may hold values from -0.125 to 0.125
- gate_weight: float32 [2048, 2048], P('fs', 'tp'), may hold values from -0.125 to 0.125
- x_scale: float32 [2048], P('tp'), may hold values from 0.5 to 2
- gate_scale: float32 [2048], P('tp'), may hold values from 0.5 to 2
- conv_weight: float32 [4, 2048], P(None, 'tp'), may hold values from -3 to 3
- recur_map: bfloat16 [2048, 32], P('tp'), may hold values from -1 to 1
- input_map: bfloat16 [2048, 32], P('tp'), may hold values from -1 to 1
- decay_param: float32 [2048], P('tp'), may hold values from 3.9 to 10
- out_weight: float32 [2048, 2048], P('tp', 'fs'), may hold values from -0.125 to 0.125
- out_scale: float32 [2048], P('fs'), may hold values from 0.5 to 2
- up_weight: float32 [2048, 6144], P('fs', 'tp'), may hold values from -0.125 to 0.125
- up_scale: float32 [6144], P('tp'), may hold values from 0.5 to 2
- down_weight: float32 [6144, 2048], P('tp', 'fs'), may hold values from -0.078125 to 0.078125
- down_scale: float32 [2048], P('fs'), may hold values from 0.5 to 2
Outputs:
- layer_out: bfloat16 [16, 512, 2048], P(('rep', 'fs'), 'tp')
The draws below stay inside these ranges and needn't reach their ends.
All inputs are finite; a program needn't handle non-finite values.
Results may differ from the reference program's by a relative error of at most 0.025.
Values may be sent and summed in bfloat16 or wider, within the bound.
No kernel may reach another device: no remote copies, remote signals or barrier semaphores. Data moves between devices by JAX's collectives and lax.ppermute only.
A program may use at most 128 MiB of HBM per device.

```python
import math
import jax
import jax.numpy as jnp
from jax import lax

D = 2048
W = 2048
FF = 6144
BLOCK = 32
CONV = 4
SEQ = 512
SEQS = 16
N_TP = 2


def draw_decay_param(key, part):
    keys = jax.random.split(jax.random.fold_in(key, 11), 2)
    slow_share = 0.5
    chooser = jax.random.uniform(keys[0], (W,), jnp.float32)
    spread = jax.random.uniform(keys[1], (W,), jnp.float32)
    slow_rate = jnp.minimum(jnp.exp(jnp.log(0.05 / SEQ) + spread * jnp.log(10.0)), 0.02)
    fast_rate = jnp.exp(jnp.log(0.004) + spread * jnp.log(5.0))
    rate = jnp.where(chooser < slow_share, slow_rate, fast_rate)
    return (-jnp.log(jnp.expm1(rate))).astype(jnp.float32)


def block_scale(key, shape, shards, low, largest):
    gain, own = 1.0, jax.random.fold_in(key, 6)
    for axis_at, blocks in shards:
        draws = jnp.exp(jax.random.uniform(jax.random.fold_in(own, axis_at), (blocks,), jnp.float32, low / len(shards), largest / len(shards)))
        gain = gain * jnp.repeat(draws, shape[axis_at] // blocks).reshape([-1 if axis == axis_at else 1 for axis in range(len(shape))])
    return gain


def normal_values(stream_key, shape, deviation, bound, cuts=(), dtype=jnp.bfloat16):
    level = block_scale(stream_key, shape, cuts, -0.22, 0.18) if cuts else 1.0
    result = jax.random.normal(stream_key, shape, jnp.float32) * deviation * level
    return jnp.minimum(jnp.maximum(result, -bound), bound).astype(dtype)


def setup_inputs(seed: int = 0) -> dict:
    streams_of = jax.random.split(jax.random.key(seed), 20)
    tokens = normal_values(streams_of[0], (SEQS, SEQ, D), 1.0, 6.0, ((0, 16),))
    gain_mix_pre = jnp.clip(1.0 + 0.18 * jax.random.normal(streams_of[1], (D,), jnp.float32), 0.1, 1.9)
    gain_mix_post = jnp.clip(1.0 + 0.18 * jax.random.normal(streams_of[2], (D,), jnp.float32), 0.1, 1.9)
    gain_mlp_pre = jnp.clip(1.0 + 0.18 * jax.random.normal(streams_of[3], (D,), jnp.float32), 0.1, 1.9)
    gain_mlp_post = jnp.clip(1.0 + 0.18 * jax.random.normal(streams_of[4], (D,), jnp.float32), 0.1, 1.9)
    x_weight = normal_values(streams_of[5], (D, W), D ** -0.5, 0.125, ((0, 8), (1, 2)), jnp.float32)
    gate_weight = normal_values(streams_of[6], (D, W), D ** -0.5, 0.125, ((0, 8), (1, 2)), jnp.float32)
    x_scale = jnp.clip(jnp.exp(math.log(2.0) - 1.3862944 * jax.random.uniform(streams_of[7], (W,), jnp.float32) ** block_scale(streams_of[7], (W,), ((0, 2),), -0.2, 0.2)), 0.5, 2.0)
    gate_scale = jnp.clip(jnp.exp(math.log(2.0) - 1.3862944 * jax.random.uniform(streams_of[8], (W,), jnp.float32) ** block_scale(streams_of[8], (W,), ((0, 2),), -0.2, 0.2)), 0.5, 2.0)
    conv_weight = normal_values(streams_of[9], (CONV, W), 0.5, 3.0, ((1, 2),), jnp.float32)
    recur_map = normal_values(streams_of[10], (W, BLOCK), BLOCK ** -0.5, 1.0, ((0, 2),))
    input_map = normal_values(streams_of[11], (W, BLOCK), BLOCK ** -0.5, 1.0, ((0, 2),))
    decay_param = draw_decay_param(jax.random.fold_in(streams_of[19], 71), 0)
    out_weight = normal_values(streams_of[13], (W, D), W ** -0.5, 0.125, ((0, 2), (1, 8)), jnp.float32)
    out_scale = jnp.clip(jnp.exp(math.log(2.0) - 1.3862944 * jax.random.uniform(streams_of[14], (D,), jnp.float32) ** block_scale(streams_of[14], (D,), ((0, 8),), -0.2, 0.2)), 0.5, 2.0)
    up_weight = normal_values(streams_of[15], (D, FF), D ** -0.5, 0.125, ((0, 8), (1, 2)), jnp.float32)
    up_scale = jnp.clip(jnp.exp(math.log(2.0) - 1.3862944 * jax.random.uniform(streams_of[16], (FF,), jnp.float32) ** block_scale(streams_of[16], (FF,), ((0, 2),), -0.2, 0.2)), 0.5, 2.0)
    down_weight = normal_values(streams_of[17], (FF, D), FF ** -0.5, 0.078125, ((0, 2), (1, 8)), jnp.float32)
    down_scale = jnp.clip(jnp.exp(math.log(2.0) - 1.3862944 * jax.random.uniform(streams_of[18], (D,), jnp.float32) ** block_scale(streams_of[18], (D,), ((0, 8),), -0.2, 0.2)), 0.5, 2.0)
    return dict(tokens=tokens, gain_mix_pre=gain_mix_pre, gain_mix_post=gain_mix_post, gain_mlp_pre=gain_mlp_pre, gain_mlp_post=gain_mlp_post, x_weight=x_weight, gate_weight=gate_weight, x_scale=x_scale, gate_scale=gate_scale, conv_weight=conv_weight, recur_map=recur_map, input_map=input_map, decay_param=decay_param, out_weight=out_weight, out_scale=out_scale, up_weight=up_weight, up_scale=up_scale, down_weight=down_weight, down_scale=down_scale)


EPSILON = 1e-06
DECAY_SCALE = 8.0

def rms_rows(values, gain_vector):
    return values * lax.rsqrt(lax.optimization_barrier(jnp.mean(values * values, axis=-1, keepdims=True)) + EPSILON) * gain_vector

def link_states(earlier, later):
    return (earlier[0] * later[0], later[0] * earlier[1] + later[1])

def reference(tokens, gain_mix_pre, gain_mix_post, gain_mlp_pre, gain_mlp_post, x_weight, gate_weight, x_scale, gate_scale, conv_weight, recur_map, input_map, decay_param, out_weight, out_scale, up_weight, up_scale, down_weight, down_scale):
    x_bf = x_weight.astype(jnp.bfloat16)
    gate_bf = gate_weight.astype(jnp.bfloat16)
    out_bf = out_weight.astype(jnp.bfloat16)
    up_bf = up_weight.astype(jnp.bfloat16)
    down_bf = down_weight.astype(jnp.bfloat16)
    blocks = W // BLOCK
    recur_blocks = recur_map.astype(jnp.float32).reshape(blocks, BLOCK, BLOCK)
    input_blocks = input_map.astype(jnp.float32).reshape(blocks, BLOCK, BLOCK)
    hidden_group = FF // N_TP
    channel_group = W // N_TP

    def one_sequence(seq_tokens):
        resid_in = seq_tokens.astype(jnp.float32)
        normed = rms_rows(resid_in, gain_mix_pre).astype(jnp.bfloat16)
        x_branch = (jnp.dot(normed, x_bf, preferred_element_type=jnp.float32) * x_scale).astype(jnp.bfloat16)
        gate_branch = (jnp.dot(normed, gate_bf, preferred_element_type=jnp.float32) * gate_scale).astype(jnp.bfloat16)
        padded = jnp.concatenate([jnp.zeros((CONV - 1, W), jnp.bfloat16), x_branch], axis=0)
        conv_sum = jnp.zeros((SEQ, W), jnp.float32)
        for tap_index in range(CONV):
            conv_sum = conv_sum + conv_weight[tap_index] * padded[tap_index:tap_index + SEQ].astype(jnp.float32)
        conv_out = lax.optimization_barrier(conv_sum.astype(jnp.bfloat16)).astype(jnp.float32)
        conv_blocks = conv_out.reshape(SEQ, blocks, BLOCK)
        recur_logit = jnp.einsum('tnc,ncd->tnd', conv_blocks, recur_blocks, precision=lax.Precision.HIGHEST).reshape(SEQ, W)
        input_logit = jnp.einsum('tnc,ncd->tnd', conv_blocks, input_blocks, precision=lax.Precision.HIGHEST).reshape(SEQ, W)
        log_decay = -DECAY_SCALE * jax.nn.sigmoid(recur_logit) * jax.nn.softplus(-decay_param)
        drive = jnp.sqrt(-jnp.expm1(2.0 * log_decay)) * jax.nn.sigmoid(input_logit) * conv_out
        _, states = lax.associative_scan(link_states, (jnp.exp(log_decay), drive), axis=0)
        mixed = (states * jax.nn.gelu(gate_branch.astype(jnp.float32))).astype(jnp.bfloat16)
        mix_sum = jnp.zeros((SEQ, D), jnp.float32)
        for group_index in range(N_TP):
            first_col = group_index * channel_group
            mix_part = jnp.dot(mixed[:, first_col:first_col + channel_group], out_bf[first_col:first_col + channel_group], preferred_element_type=jnp.float32) * out_scale
            mix_sum = mix_sum + lax.optimization_barrier(mix_part.astype(jnp.bfloat16)).astype(jnp.float32)
        hidden_state = (resid_in + rms_rows(mix_sum, gain_mix_post)).astype(jnp.bfloat16)
        normed_mlp = rms_rows(hidden_state.astype(jnp.float32), gain_mlp_pre).astype(jnp.bfloat16)
        up_proj = jnp.dot(normed_mlp, up_bf, preferred_element_type=jnp.float32) * up_scale
        activated = jnp.square(jax.nn.relu(up_proj)).astype(jnp.bfloat16)
        mlp_sum = jnp.zeros((SEQ, D), jnp.float32)
        for group_index in range(N_TP):
            first_col = group_index * hidden_group
            partial_value = jnp.dot(activated[:, first_col:first_col + hidden_group], down_bf[first_col:first_col + hidden_group], preferred_element_type=jnp.float32) * down_scale
            mlp_sum = mlp_sum + lax.optimization_barrier(partial_value.astype(jnp.bfloat16)).astype(jnp.float32)
        return (hidden_state.astype(jnp.float32) + rms_rows(mlp_sum, gain_mlp_post)).astype(jnp.bfloat16)
    return lax.map(one_sequence, tokens)
```

```python
import functools

import jax
import jax.numpy as jnp
import numpy as np
from jax import lax
from jax.experimental import pallas as pl
from jax.experimental.pallas import tpu as pltpu
from jax.sharding import PartitionSpec as P

BLOCK = 32
EPSILON = 1e-06
DECAY_SCALE = 8.0
BF16 = jnp.bfloat16
F32 = jnp.float32
LANES = 128
TIME_PAD = 8
VMEM_LIMIT = 56 * 1024 * 1024


def rms_rows(values, gain_vector):
    return (
        values
        * lax.rsqrt(jnp.mean(values * values, axis=-1, keepdims=True) + EPSILON)
        * gain_vector
    )


def params(**kw):
    return pltpu.CompilerParams(vmem_limit_bytes=VMEM_LIMIT, **kw)


def cost(flops, bytes_accessed, transcendentals=0):
    return pl.CostEstimate(
        flops=int(flops), bytes_accessed=int(bytes_accessed), transcendentals=int(transcendentals)
    )


def whole_spec(shape):
    zeros = (0,) * len(shape)
    return pl.BlockSpec(shape, lambda *_: zeros)


def ring_order(count):
    return list(range(0, count, 2)) + [i for i in range(count - 1, 0, -1) if i % 2]


def ring_tables(count):
    ring = ring_order(count)
    place = {dev: i for i, dev in enumerate(ring)}
    table = np.zeros((count, 2 * count), np.int32)
    for dev in range(count):
        for s in range(count):
            table[dev, s] = ring[(place[dev] - s) % count]
            table[dev, count + s] = ring[(place[dev] + s) % count]
    return table


def ring_perms(count):
    ring = ring_order(count)
    fwd = [(ring[i], ring[(i + 1) % count]) for i in range(count)]
    return fwd, [(b, a) for a, b in fwd]


def ring_pair(name, first, second, count):
    fwd, bwd = ring_perms(count)
    a, b = [first], [second]
    for s in range(1, count):
        with jax.named_scope(f"{name}_f{s}"):
            a.append(lax.ppermute(a[-1], "fs", fwd))
        with jax.named_scope(f"{name}_b{s}"):
            b.append(lax.ppermute(b[-1], "fs", bwd))
    return a, b


def shift(value, axis, count, by):
    return lax.ppermute(value, axis, [((i + by) % count, i) for i in range(count)])


def gather_small(value, axis, count, index):
    if count & (count - 1):
        return lax.all_gather(value, axis, axis=value.ndim - 1, tiled=True)
    step = 1
    while step < count:
        other = lax.ppermute(value, axis, [(i, i ^ step) for i in range(count)])
        low = (index & step) == 0
        value = jnp.where(
            low,
            jnp.concatenate([value, other], axis=-1),
            jnp.concatenate([other, value], axis=-1),
        )
        step *= 2
    return value


def project_kernel(steps, order, tokens, x_scale, gate_scale, *refs):
    xs, gs = refs[:steps], refs[steps : 2 * steps]
    x_out, gate_out, normed = refs[2 * steps :]
    rows = xs[0].shape[0]
    v = tokens[...].astype(F32)
    normed[...] = (
        v * lax.rsqrt(jnp.mean(v * v, axis=-1, keepdims=True) + EPSILON)
    ).astype(BF16)
    for way, (chunks, scale, out) in enumerate(
        ((xs, x_scale, x_out), (gs, gate_scale, gate_out))
    ):
        total = None
        for s in range(steps):
            at = pl.multiple_of(order[way * steps + s] * rows, rows)
            part = jnp.dot(
                normed[:, pl.ds(at, rows)], chunks[s][...], preferred_element_type=F32
            )
            total = part if total is None else total + part
        out[...] = (total * scale[...]).astype(BF16)


def project(order, tokens, x_scale, gate_scale, xs, gs):
    steps = len(xs)
    length, width = tokens.shape
    cols = xs[0].shape[1]
    tile = 256 if length % 256 == 0 else length
    row = lambda n: pl.BlockSpec((tile, n), lambda i, *_: (i, 0))
    out = jax.ShapeDtypeStruct((length, cols), BF16)
    return pl.pallas_call(
        functools.partial(project_kernel, steps),
        grid_spec=pltpu.PrefetchScalarGridSpec(
            num_scalar_prefetch=1,
            grid=(length // tile,),
            in_specs=[row(width), whole_spec((1, cols)), whole_spec((1, cols))]
            + [whole_spec(xs[0].shape)] * (2 * steps),
            out_specs=[row(cols), row(cols)],
            scratch_shapes=[pltpu.VMEM((tile, width), BF16)],
        ),
        out_shape=[out, out],
        compiler_params=params(),
        cost_estimate=cost(4 * length * width * cols, 2 * (length + 2 * cols) * width),
        name="project",
    )(order, tokens, x_scale, gate_scale, *xs, *gs)


def recur_kernel(x_ref, gate_ref, conv_ref, maps_ref, rate_ref, out_ref, pad, decay, state):
    seqs, length, width = x_ref.shape
    blocks = width // LANES
    lines = seqs * blocks
    stride = length + TIME_PAD
    taps = conv_ref.shape[0]
    pad[0:TIME_PAD, :] = jnp.zeros((TIME_PAD, LANES), F32)
    for q in range(seqs):
        for b in range(blocks):
            cols = slice(b * LANES, (b + 1) * LANES)
            base = (q * blocks + b) * stride
            pad[TIME_PAD:, :] = x_ref[q, :, cols].astype(F32)
            total = None
            for k in range(taps):
                at = TIME_PAD - (taps - 1) + k
                part = conv_ref[k : k + 1, cols] * pad[at : at + length, :]
                total = part if total is None else total + part
            conv = total.astype(BF16)
            logits = jnp.dot(conv, maps_ref[b], preferred_element_type=F32)
            log_decay = rate_ref[:, cols] * jax.nn.sigmoid(logits[:, :LANES])
            a = jnp.exp(log_decay)
            y = 2.0 * log_decay
            series = -y * (
                1.0
                + y * (1 / 2 + y * (1 / 6 + y * (1 / 24 + y * (1 / 120 + y * (1 / 720)))))
            )
            loss = jnp.where(y > -0.4, series, 1.0 - a * a)
            decay[base : base + length, :] = a
            state[base : base + length, :] = (
                jnp.sqrt(loss) * jax.nn.sigmoid(logits[:, LANES:]) * conv.astype(F32)
            )

    def advance(t, h):
        at = pl.ds(t, lines, stride=stride)
        h = decay[at, :] * h + state[at, :]
        state[at, :] = h
        return h

    lax.fori_loop(0, length, advance, jnp.zeros((lines, LANES), F32), unroll=16)
    for q in range(seqs):
        for b in range(blocks):
            cols = slice(b * LANES, (b + 1) * LANES)
            base = (q * blocks + b) * stride
            g = gate_ref[q, :, cols].astype(F32)
            out_ref[q, :, cols] = (
                state[base : base + length, :] * jax.nn.gelu(g)
            ).astype(BF16)


def recur(x_branch, gate_branch, conv_weight, maps, rate):
    seqs, length, width = x_branch.shape
    lines = seqs * (width // LANES)
    rows = lines * (length + TIME_PAD)
    vmem = pl.BlockSpec(memory_space=pltpu.VMEM)
    return pl.pallas_call(
        recur_kernel,
        in_specs=[vmem] * 5,
        out_specs=vmem,
        out_shape=jax.ShapeDtypeStruct(x_branch.shape, BF16),
        scratch_shapes=[
            pltpu.VMEM((length + TIME_PAD, LANES), F32),
            pltpu.VMEM((rows, LANES), F32),
            pltpu.VMEM((rows, LANES), F32),
        ],
        compiler_params=params(),
        cost_estimate=cost(3e9, 6 * x_branch.size, 10 * x_branch.size),
        name="recur",
    )(x_branch, gate_branch, conv_weight, maps, rate)


def out_kernel(steps, order, mixed, *refs):
    top, low = refs[:steps], refs[steps : 2 * steps]
    out = refs[2 * steps]
    half, cols = top[0].shape
    for s in range(steps):
        at = pl.multiple_of(order[s] * cols, cols)
        part = jnp.dot(mixed[0, :, :half], top[s][...], preferred_element_type=F32)
        part = part + jnp.dot(
            mixed[0, :, half:], low[(steps - s) % steps][...], preferred_element_type=F32
        )
        out[0, :, pl.ds(at, cols)] = part.astype(BF16)


def out_project(order, piece, mixed, share, top, low):
    steps = len(top)
    seqs, length, width = mixed.shape
    cols = steps * top[0].shape[1]
    scalars = jnp.concatenate([order, piece.reshape(1)])
    return pl.pallas_call(
        functools.partial(out_kernel, steps),
        grid_spec=pltpu.PrefetchScalarGridSpec(
            num_scalar_prefetch=1,
            grid=(seqs,),
            in_specs=[pl.BlockSpec((1, share, width), lambda i, s: (i, s[2 * steps], 0))]
            + [whole_spec(top[0].shape)] * (2 * steps),
            out_specs=pl.BlockSpec((1, share, cols), lambda i, *_: (i, 0, 0)),
        ),
        out_shape=jax.ShapeDtypeStruct((seqs, share, cols), BF16),
        compiler_params=params(),
        cost_estimate=cost(
            2 * seqs * share * width * cols, 2 * (width * cols + seqs * share * (width + cols))
        ),
        name="out_project",
    )(scalars, mixed, *top, *low)


def mid_kernel(parts, tokens, gain, *refs):
    hidden, normed = refs[parts:]
    total = refs[0][...].astype(F32)
    for i in range(1, parts):
        total = total + refs[i][...].astype(F32)
    h = (
        tokens[...].astype(F32)
        + total
        * lax.rsqrt(jnp.mean(total * total, axis=-1, keepdims=True) + EPSILON)
        * gain[...]
    ).astype(BF16)
    hidden[...] = h
    v = h.astype(F32)
    normed[...] = (
        v * lax.rsqrt(jnp.mean(v * v, axis=-1, keepdims=True) + EPSILON)
    ).astype(BF16)


def mid(tokens, gain, parts):
    rows, width = tokens.shape
    tile = rows // 2
    row = pl.BlockSpec((tile, width), lambda i: (i, 0))
    out = jax.ShapeDtypeStruct((rows, width), BF16)
    return pl.pallas_call(
        functools.partial(mid_kernel, len(parts)),
        grid=(rows // tile,),
        in_specs=[row, whole_spec((1, width))] + [row] * len(parts),
        out_specs=[row, row],
        out_shape=[out, out],
        compiler_params=params(),
        cost_estimate=cost(2e9, 2 * rows * width * (3 + len(parts))),
        name="mid",
    )(tokens, gain, *parts)


def up_kernel(steps, ways, blocks, order, scale, *refs):
    chunks = [refs[w * steps : (w + 1) * steps] for w in range(len(ways))]
    xs = refs[len(ways) * steps : len(ways) * steps + blocks]
    out = refs[-1]
    rows, cols = chunks[0][0].shape
    for i in range(blocks):
        for w, way in enumerate(ways):
            total = None
            for s in range(steps):
                at = pl.multiple_of(order[way * steps + s] * rows, rows)
                part = jnp.dot(
                    xs[i][:, pl.ds(at, rows)], chunks[w][s][...], preferred_element_type=F32
                )
                total = part if total is None else total + part
            span = slice(w * cols, (w + 1) * cols)
            total = jnp.maximum(total * scale[:, span], 0.0)
            out[i, :, span] = (total * total).astype(BF16)


def up_project(order, scale, streams, xs):
    steps = len(streams[0][1])
    ways = tuple(way for way, _ in streams)
    rows, width = xs[0].shape
    cols = streams[0][1][0].shape[1] * len(streams)
    vmem = pl.BlockSpec(memory_space=pltpu.VMEM)
    flat = [c for _, chunks in streams for c in chunks]
    return pl.pallas_call(
        functools.partial(up_kernel, steps, ways, len(xs)),
        grid_spec=pltpu.PrefetchScalarGridSpec(
            num_scalar_prefetch=1,
            grid=(),
            in_specs=[vmem] * (1 + len(flat) + len(xs)),
            out_specs=vmem,
        ),
        out_shape=jax.ShapeDtypeStruct((len(xs), rows, cols), BF16),
        compiler_params=params(),
        cost_estimate=cost(
            2 * len(xs) * rows * width * cols,
            2 * (width * cols + len(xs) * rows * (width + cols)),
        ),
        name="up_project",
    )(order, scale, *flat, *xs)


def down_kernel(steps, depth, acts, *refs):
    a, chunks, outs = refs[:acts], refs[acts : acts + steps * 2 * depth], refs[acts + steps * 2 * depth :]
    part_rows, cols = chunks[0].shape
    for s in range(steps):
        for way in range(2):
            for d, act in enumerate(a):
                for i in range(act.shape[0]):
                    total = None
                    for k in range(depth):
                        part = jnp.dot(
                            act[i, :, k * part_rows : (k + 1) * part_rows],
                            chunks[(s * 2 + way) * depth + k][...],
                            preferred_element_type=F32,
                        )
                        total = part if total is None else total + part
                    at = (s * 2 + way) * cols
                    outs[i][d, :, at : at + cols] = total.astype(BF16)


def down_project(acts, pieces):
    steps, depth = len(pieces), len(pieces[0][0])
    blocks, rows, hidden = acts[0].shape
    flat = [c for step in pieces for way in step for c in way]
    cols = flat[0].shape[1] * 2 * steps
    vmem = pl.BlockSpec(memory_space=pltpu.VMEM)
    return pl.pallas_call(
        functools.partial(down_kernel, steps, depth, len(acts)),
        in_specs=[vmem] * (len(acts) + len(flat)),
        out_specs=[vmem] * blocks,
        out_shape=[jax.ShapeDtypeStruct((len(acts), rows, cols), BF16)] * blocks,
        compiler_params=params(),
        cost_estimate=cost(
            2 * len(acts) * blocks * rows * hidden * cols,
            2 * (hidden * cols + len(acts) * blocks * rows * (hidden + cols)),
        ),
        name="down_project",
    )(*acts, *flat)


def last_kernel(groups, parts, count, order, hidden, gain, *refs):
    out, total = refs[-2:]
    rows, width = hidden.shape
    half = width // count // 2
    step = 0
    for g, steps in enumerate(groups):
        mine = refs[g * parts : (g + 1) * parts]
        for s in range(steps):
            for way in range(2):
                at = (s * 2 + way) * half
                value = mine[0][0, :, at : at + half].astype(F32)
                for ref in mine[1:]:
                    value = value + ref[0, :, at : at + half].astype(F32)
                to = pl.multiple_of(order[way * count + step] * (2 * half) + way * half, half)
                total[:, pl.ds(to, half)] = value
            step += 1
    v = total[...]
    out[...] = (
        hidden[...].astype(F32)
        + v * lax.rsqrt(jnp.mean(v * v, axis=-1, keepdims=True) + EPSILON) * gain[...]
    ).astype(BF16)


def last(order, hidden, gain, groups, parts):
    rows, width = hidden.shape
    tile = rows // 2
    flat = [p for group in parts for p in group]
    row = pl.BlockSpec((tile, width), lambda i, *_: (i, 0))
    return pl.pallas_call(
        functools.partial(last_kernel, groups, len(parts[0]), order.shape[0] // 2),
        grid_spec=pltpu.PrefetchScalarGridSpec(
            num_scalar_prefetch=1,
            grid=(rows // tile,),
            in_specs=[row, whole_spec((1, width))]
            + [pl.BlockSpec((1, tile, p.shape[2]), lambda i, *_: (0, i, 0)) for p in flat],
            out_specs=row,
            scratch_shapes=[pltpu.VMEM((tile, width), F32)],
        ),
        out_shape=jax.ShapeDtypeStruct((rows, width), BF16),
        compiler_params=params(),
        cost_estimate=cost(1e9, 2 * rows * width * (2 + len(parts[0]))),
        name="last",
    )(order, hidden, gain, *flat)


GROUPS = (4, 2, 1, 1)
UP_SPLIT = 2
DOWN_SPLIT = 2


def group_sizes(count):
    if count == sum(GROUPS):
        return GROUPS
    return (count - 2, 1, 1) if count > 2 else (count,)


def ring_device(
    reps,
    count,
    tps,
    tokens,
    gain_mix_pre,
    gain_mix_post,
    gain_mlp_pre,
    gain_mlp_post,
    x_weight,
    gate_weight,
    x_scale,
    gate_scale,
    conv_weight,
    recur_map,
    input_map,
    decay_param,
    out_weight,
    out_scale,
    up_weight,
    up_scale,
    down_weight,
    down_scale,
):
    rep, me, tp = (lax.axis_index(a) for a in ("rep", "fs", "tp"))
    length, width = tokens.shape[1:]
    share = length // tps
    chan = x_weight.shape[1] // reps
    hid = up_weight.shape[1] // reps
    order = lax.dynamic_slice_in_dim(jnp.asarray(ring_tables(count)), me, 1, 0)[0]

    mine = lax.dynamic_slice_in_dim(tokens[0], tp * share, share, 0)
    seqs = [tokens[0]]
    for dr in range(1, reps):
        with jax.named_scope(f"tok_x{dr}"):
            got = shift(mine, "rep", reps, dr)
        seq = lax.dynamic_update_slice_in_dim(
            jnp.zeros((length, width), BF16), got, tp * share, 0
        )
        for dt in range(1, tps):
            with jax.named_scope(f"tok_t{dr}_{dt}"):
                other = shift(got, "tp", tps, dt)
            seq = lax.dynamic_update_slice_in_dim(seq, other, (tp + dt) % tps * share, 0)
        seqs.append(seq)
    rows_in = jnp.concatenate(seqs, axis=0)

    def rep_part(value, size, axis):
        return lax.dynamic_slice_in_dim(value, rep * size, size, axis)

    pre = gain_mix_pre[:, None]
    xs, gs = ring_pair(
        "ringa",
        (rep_part(x_weight, chan, 1) * pre).astype(BF16),
        (rep_part(gate_weight, chan, 1) * pre).astype(BF16),
        count,
    )
    out_mine = (rep_part(out_weight, chan, 0) * out_scale).astype(BF16)
    top, low = ring_pair("ringb", out_mine[: chan // 2], out_mine[chan // 2 :], count)

    up_mine = (rep_part(up_weight, hid, 1) * gain_mlp_pre[:, None]).astype(BF16)
    piece = hid // (2 * UP_SPLIT)
    up_streams = []
    for k in range(UP_SPLIT):
        f, b = ring_pair(
            f"ringc{k}",
            up_mine[:, 2 * k * piece : (2 * k + 1) * piece],
            up_mine[:, (2 * k + 1) * piece : (2 * k + 2) * piece],
            count,
        )
        up_streams += [(0, f), (1, b)]
    down_mine = (rep_part(down_weight, hid, 0) * down_scale).astype(BF16)
    half = down_mine.shape[1] // 2
    deep = hid // DOWN_SPLIT
    down_rings = [
        ring_pair(
            f"ringd{k}",
            down_mine[k * deep : (k + 1) * deep, :half],
            down_mine[k * deep : (k + 1) * deep, half:],
            count,
        )
        for k in range(DOWN_SPLIT)
    ]
    with jax.named_scope("gains"):
        gains = gather_small(jnp.stack([gain_mix_post, gain_mlp_post]), "fs", count, me)

    x_branch, gate_branch = project(
        order,
        rows_in,
        rep_part(x_scale, chan, 0)[None],
        rep_part(gate_scale, chan, 0)[None],
        xs,
        gs,
    )
    same = jnp.asarray(
        (np.arange(LANES)[:, None] // BLOCK == np.arange(LANES)[None] // BLOCK), BF16
    )

    def dense_map(value):
        blocks = rep_part(value, chan, 0).reshape(chan // LANES, LANES, BLOCK)
        return jnp.tile(blocks, (1, 1, LANES // BLOCK)) * same

    maps = jnp.concatenate([dense_map(recur_map), dense_map(input_map)], axis=2)
    rate = -DECAY_SCALE * jax.nn.softplus(-rep_part(decay_param, chan, 0))[None]
    mixed = recur(
        x_branch.reshape(reps, length, chan),
        gate_branch.reshape(reps, length, chan),
        rep_part(conv_weight, chan, 1),
        maps,
        rate,
    )

    def scatter_sum(parts, name):
        got = []
        for dt in range(1, tps):
            with jax.named_scope(f"{name}_t{dt}"):
                got.append(shift(parts[dt], "tp", tps, tps - dt))
        pieces = [parts[0]] + got
        for dr in range(1, reps):
            send = parts[0][dr : dr + 1].astype(F32)
            for g in got:
                send = send + g[dr : dr + 1].astype(F32)
            with jax.named_scope(f"{name}_x{dr}"):
                pieces.append(shift(send.astype(BF16), "rep", reps, reps - dr))
        return pieces

    parts = [None] * tps
    for dt in reversed(range(tps)):
        parts[dt] = out_project(order, (tp + dt) % tps, mixed, share, top, low)
    mix_pieces = scatter_sum(parts, "mix")
    hidden, normed = mid(mine, gains[0:1], [p[0] for p in mix_pieces])

    scale = rep_part(up_scale, hid, 0)[None]
    acts = []
    for dr in range(reps):
        with jax.named_scope(f"mlp_x{dr}"):
            base = shift(normed, "rep", reps, dr) if dr else normed
        blocks = [base]
        for dt in range(1, tps):
            with jax.named_scope(f"mlp_t{dr}_{dt}"):
                blocks.append(shift(base, "tp", tps, dt))
        acts.append(up_project(order, scale, up_streams, blocks))

    groups = group_sizes(count)
    sums, first = [], 0
    for g, steps in enumerate(groups):
        pieces = [
            [[ring[way][s] for ring in down_rings] for way in range(2)]
            for s in range(first, first + steps)
        ]
        first += steps
        sums.append(scatter_sum(down_project(acts, pieces), f"mlp{g}"))
    return last(order, hidden, gains[1:2], groups, sums)[None]


def link_states(earlier, later):
    return (earlier[0] * later[0], later[0] * earlier[1] + later[1])


def plain_device(
    tokens,
    gain_mix_pre,
    gain_mix_post,
    gain_mlp_pre,
    gain_mlp_post,
    x_weight,
    gate_weight,
    x_scale,
    gate_scale,
    conv_weight,
    recur_map,
    input_map,
    decay_param,
    out_weight,
    out_scale,
    up_weight,
    up_scale,
    down_weight,
    down_scale,
):
    resid_in = tokens[0].astype(F32)
    length = resid_in.shape[0]
    local_width = x_weight.shape[1]
    gains = lax.all_gather(
        jnp.stack(
            [gain_mix_pre, gain_mix_post, gain_mlp_pre, gain_mlp_post, out_scale, down_scale]
        ),
        "fs",
        axis=1,
        tiled=True,
    )
    gather = lambda w, axis: lax.all_gather(w.astype(BF16), "fs", axis=axis, tiled=True)
    normed = rms_rows(resid_in, gains[0]).astype(BF16)
    x_proj = jnp.dot(normed, gather(x_weight, 0), preferred_element_type=F32)
    gate_proj = jnp.dot(normed, gather(gate_weight, 0), preferred_element_type=F32)
    out_cols = gather(out_weight, 1)
    down_full = gather(down_weight, 1)
    x_branch = (x_proj * x_scale).astype(BF16)
    gate_branch = (gate_proj * gate_scale).astype(BF16)
    taps = conv_weight.shape[0]
    padded = jnp.concatenate([jnp.zeros((taps - 1, local_width), BF16), x_branch], axis=0)
    conv_sum = conv_weight[0] * padded[0:length].astype(F32)
    for k in range(1, taps):
        conv_sum = conv_sum + conv_weight[k] * padded[k : k + length].astype(F32)
    conv_out = lax.optimization_barrier(conv_sum.astype(BF16))
    blocks = local_width // BLOCK
    conv_blocks = conv_out.reshape(length, blocks, BLOCK)

    def logits(value):
        return jnp.einsum(
            "tnc,ncd->tnd",
            conv_blocks,
            value.reshape(blocks, BLOCK, BLOCK),
            preferred_element_type=F32,
        ).reshape(length, local_width)

    log_decay = (
        -DECAY_SCALE * jax.nn.sigmoid(logits(recur_map)) * jax.nn.softplus(-decay_param)
    )
    drive = (
        jnp.sqrt(-jnp.expm1(2.0 * log_decay))
        * jax.nn.sigmoid(logits(input_map))
        * conv_out.astype(F32)
    )
    _, states = lax.associative_scan(link_states, (jnp.exp(log_decay), drive), axis=0)
    mixed = (states * jax.nn.gelu(gate_branch.astype(F32))).astype(BF16)
    share_rows = length // lax.axis_size("tp")

    def scatter(left, right, scale):
        part = (jnp.dot(left, right, preferred_element_type=F32) * scale).astype(BF16)
        return lax.psum_scatter(part, "tp", scatter_dimension=0, tiled=True).astype(F32)

    mix_share = scatter(mixed, out_cols, gains[4])
    resid_share = lax.dynamic_slice_in_dim(
        resid_in, lax.axis_index("tp") * share_rows, share_rows, 0
    )
    hidden_state = (resid_share + rms_rows(mix_share, gains[1])).astype(BF16)
    normed_mlp = rms_rows(hidden_state.astype(F32), gains[2]).astype(BF16)
    mlp_input = lax.all_gather(normed_mlp, "tp", axis=0, tiled=True)
    up_proj = jnp.dot(mlp_input, gather(up_weight, 0), preferred_element_type=F32)
    activated = jnp.square(jax.nn.relu(up_proj * up_scale)).astype(BF16)
    mlp_share = scatter(activated, down_full, gains[5])
    out_share = hidden_state.astype(F32) + rms_rows(mlp_share, gains[3])
    return out_share.astype(BF16)[None]


def solution(mesh):
    in_specs = (
        P(("rep", "fs"), None, None),
        P("fs"),
        P("fs"),
        P("fs"),
        P("fs"),
        P("fs", "tp"),
        P("fs", "tp"),
        P("tp"),
        P("tp"),
        P(None, "tp"),
        P("tp", None),
        P("tp", None),
        P("tp"),
        P("tp", "fs"),
        P("fs"),
        P("fs", "tp"),
        P("tp"),
        P("tp", "fs"),
        P("fs"),
    )
    reps, count, tps = (mesh.shape[a] for a in ("rep", "fs", "tp"))

    def on_device(*args):
        tokens, x_weight, up_weight = args[0], args[5], args[15]
        length, rows = tokens.shape[1], x_weight.shape[0]
        chan, hid = x_weight.shape[1] // reps, up_weight.shape[1] // reps
        fits = (
            count % 2 == 0
            and rows % (2 * LANES) == 0
            and chan % (2 * LANES) == 0
            and hid % (2 * LANES * max(UP_SPLIT, DOWN_SPLIT)) == 0
            and length % (32 * tps) == 0
            and reps * (chan // LANES) <= 8
        )
        if fits:
            return ring_device(reps, count, tps, *args)
        return plain_device(*args)

    return jax.shard_map(
        on_device,
        mesh=mesh,
        in_specs=in_specs,
        out_specs=P(("rep", "fs"), "tp", None),
        check_vma=False,
    )
```

```python
import functools

import jax
import jax.numpy as jnp
import numpy as np
from jax import lax
from jax.experimental import pallas as pl
from jax.experimental.pallas import tpu as pltpu
from jax.sharding import PartitionSpec as P


BLOCK = 32
EPSILON = 1e-06
DECAY_SCALE = 8.0
BF16 = jnp.bfloat16
F32 = jnp.float32
LANES = 128
TIME_PAD = 8
VMEM_LIMIT = 56 * 1024 * 1024


def rms_rows(values, gain_vector):
    return (
        values
        * lax.rsqrt(jnp.mean(values * values, axis=-1, keepdims=True) + EPSILON)
        * gain_vector
    )


def params(**kw):
    return pltpu.CompilerParams(vmem_limit_bytes=VMEM_LIMIT, **kw)


def cost(flops, bytes_accessed, transcendentals=0):
    return pl.CostEstimate(
        flops=int(flops), bytes_accessed=int(bytes_accessed), transcendentals=int(transcendentals)
    )


def whole_spec(shape):
    zeros = (0,) * len(shape)
    return pl.BlockSpec(shape, lambda *_: zeros)


def ring_order(count):
    return list(range(0, count, 2)) + [i for i in range(count - 1, 0, -1) if i % 2]


def arrival(count):
    offsets = [0]
    for k in range(1, count // 2):
        offsets += [-k, k]
    return offsets + [count // 2]


def order_table(count):
    ring = ring_order(count)
    place = {dev: i for i, dev in enumerate(ring)}
    rows = [[ring[(place[m] + off) % count] for off in arrival(count)] for m in range(count)]
    return np.asarray(rows, np.int32)


def ring_gather(first, second, count):
    ring = ring_order(count)
    fwd = [(ring[i], ring[(i + 1) % count]) for i in range(count)]
    bwd = [(b, a) for a, b in fwd]
    far = count // 2
    ahead, behind = [first, second], [first, second]
    held = [(first, second)]
    for k in range(1, far + 1):
        for h in range(2):
            if k < far or h == 0:
                ahead[h] = lax.ppermute(ahead[h], "fs", fwd)
            if k < far or h == 1:
                behind[h] = lax.ppermute(behind[h], "fs", bwd)
        if k < far:
            held += [tuple(ahead), tuple(behind)]
    return held + [(ahead[0], behind[1])]


def shift(value, axis, count, by):
    return lax.ppermute(value, axis, [((i + by) % count, i) for i in range(count)])


def exchange_small(value, axis, count):
    got = [value]
    for by in range(1, count):
        got.append(shift(value, axis, count, by))
    return got


def fetch(order, chunks, weights, first, cols, sems):
    copies = []
    for s, chunk in enumerate(chunks):
        rows = chunk.shape[0]
        at = pl.multiple_of(order[s] * rows, rows)
        copies.append(
            pltpu.make_async_copy(
                chunk.at[:, 0:cols], weights.at[pl.ds(at, rows), first : first + cols], sems.at[s]
            )
        )
    for copy in copies:
        copy.start()
    return copies


def wait_all(copies):
    for copy in copies:
        copy.wait()


def norm_kernel(count, tp, *refs):
    out = refs[-1]
    for i in range(count):

        @pl.when(pl.program_id(0) == i)
        def _():
            v = refs[i][...].astype(F32)
            scale = lax.rsqrt(jnp.mean(v * v, axis=-1, keepdims=True) + EPSILON)
            out[...] = (v * scale).astype(BF16)


def normalize(tp, pieces):
    rows, width = pieces[0].shape
    count = len(pieces)
    return pl.pallas_call(
        functools.partial(norm_kernel, count),
        grid_spec=pltpu.PrefetchScalarGridSpec(
            num_scalar_prefetch=1,
            grid=(count,),
            in_specs=[whole_spec((rows, width))] * count,
            out_specs=pl.BlockSpec((rows, width), lambda i, tp: ((tp[0] + i) % count, 0)),
        ),
        out_shape=jax.ShapeDtypeStruct((count * rows, width), BF16),
        compiler_params=params(),
        cost_estimate=cost(1e9, 4 * count * rows * width),
        name="normalize",
    )(tp, *pieces)


def project_kernel(steps, order, normed, scale, *refs):
    xs, gs = refs[:steps], refs[steps : 2 * steps]
    x_out, gate_out, x_full, gate_full, sems = refs[2 * steps :]
    cols = x_out.shape[1]
    x_copies = fetch(order, xs, x_full, 0, cols, sems.at[0])
    gate_copies = fetch(order, gs, gate_full, 0, cols, sems.at[1])
    wait_all(x_copies)
    total = jnp.dot(normed[...], x_full[...], preferred_element_type=F32)
    x_out[...] = (total * scale[:, :cols]).astype(BF16)
    wait_all(gate_copies)
    total = jnp.dot(normed[...], gate_full[...], preferred_element_type=F32)
    gate_out[...] = (total * scale[:, cols:]).astype(BF16)


def project(order, normed, scale, held):
    steps = len(held)
    length, width = normed.shape
    cols = scale.shape[1] // 2
    out = jax.ShapeDtypeStruct((length, cols), BF16)
    vmem = pl.BlockSpec(memory_space=pltpu.VMEM)
    hbm = pl.BlockSpec(memory_space=pltpu.HBM)
    return pl.pallas_call(
        functools.partial(project_kernel, steps),
        grid_spec=pltpu.PrefetchScalarGridSpec(
            num_scalar_prefetch=1,
            grid=(),
            in_specs=[vmem, vmem] + [hbm] * (2 * steps),
            out_specs=[vmem, vmem],
            scratch_shapes=[
                pltpu.VMEM((width, cols), BF16),
                pltpu.VMEM((width, cols), BF16),
                pltpu.SemaphoreType.DMA((2, steps)),
            ],
        ),
        out_shape=[out, out],
        compiler_params=params(),
        cost_estimate=cost(4 * length * width * cols, 2 * (length + 2 * cols) * width),
        name="project",
    )(order, normed, scale, *[h[0] for h in held], *[h[1] for h in held])


def recur_kernel(x_ref, gate_ref, conv_ref, maps_ref, rate_ref, out_ref, pad, decay, state):
    seqs, length, width = x_ref.shape
    blocks = width // LANES
    lines = seqs * blocks
    stride = length + TIME_PAD
    taps = conv_ref.shape[0]
    pad[0:TIME_PAD, :] = jnp.zeros((TIME_PAD, LANES), F32)
    for q in range(seqs):
        for b in range(blocks):
            cols = slice(b * LANES, (b + 1) * LANES)
            base = (q * blocks + b) * stride
            pad[TIME_PAD:, :] = x_ref[q, :, cols].astype(F32)
            total = None
            for k in range(taps):
                at = TIME_PAD - (taps - 1) + k
                part = conv_ref[k : k + 1, cols] * pad[at : at + length, :]
                total = part if total is None else total + part
            conv = total.astype(BF16)
            logits = jnp.dot(conv, maps_ref[b], preferred_element_type=F32)
            log_decay = rate_ref[:, cols] * jax.nn.sigmoid(logits[:, :LANES])
            a = jnp.exp(log_decay)
            y = 2.0 * log_decay
            series = -y * (
                1.0
                + y * (1 / 2 + y * (1 / 6 + y * (1 / 24 + y * (1 / 120 + y * (1 / 720)))))
            )
            loss = jnp.where(y > -0.4, series, 1.0 - a * a)
            decay[base : base + length, :] = a
            state[base : base + length, :] = (
                jnp.sqrt(loss) * jax.nn.sigmoid(logits[:, LANES:]) * conv.astype(F32)
            )

    def advance(t, h):
        at = pl.ds(t, lines, stride=stride)
        h = decay[at, :] * h + state[at, :]
        state[at, :] = h
        return h

    lax.fori_loop(0, length, advance, jnp.zeros((lines, LANES), F32), unroll=16)
    for q in range(seqs):
        for b in range(blocks):
            cols = slice(b * LANES, (b + 1) * LANES)
            base = (q * blocks + b) * stride
            g = gate_ref[q, :, cols].astype(F32)
            out_ref[q, :, cols] = (
                state[base : base + length, :] * jax.nn.gelu(g)
            ).astype(BF16)


def recur(x_branch, gate_branch, conv_weight, maps, rate):
    seqs, length, width = x_branch.shape
    lines = seqs * (width // LANES)
    rows = lines * (length + TIME_PAD)
    vmem = pl.BlockSpec(memory_space=pltpu.VMEM)
    return pl.pallas_call(
        recur_kernel,
        in_specs=[vmem] * 5,
        out_specs=vmem,
        out_shape=jax.ShapeDtypeStruct(x_branch.shape, BF16),
        scratch_shapes=[
            pltpu.VMEM((length + TIME_PAD, LANES), F32),
            pltpu.VMEM((rows, LANES), F32),
            pltpu.VMEM((rows, LANES), F32),
        ],
        compiler_params=params(),
        cost_estimate=cost(3e9, 6 * x_branch.size, 10 * x_branch.size),
        name="recur",
    )(x_branch, gate_branch, conv_weight, maps, rate)


def out_kernel(steps, order, mixed, *refs):
    top, low = refs[:steps], refs[steps : 2 * steps]
    outs = refs[2 * steps :]
    tps, share = len(outs), outs[0].shape[1]
    half, cols = top[0].shape
    pieces = []
    for j in range(tps):
        at = pl.multiple_of((order[steps] + j) % tps * share, share)
        pieces.append(mixed[0, pl.ds(at, share), :])
    m = jnp.concatenate(pieces, axis=0)
    for s in range(steps):
        at = pl.multiple_of(order[s] * cols, cols)
        part = jnp.dot(m[:, :half], top[s][...], preferred_element_type=F32)
        part = part + jnp.dot(m[:, half:], low[s][...], preferred_element_type=F32)
        for j, out in enumerate(outs):
            out[0, :, pl.ds(at, cols)] = part[j * share : (j + 1) * share].astype(BF16)


def out_project(order, tp, tps, mixed, held, cols):
    steps = len(held)
    seqs, length, width = mixed.shape
    share = length // tps
    scalars = jnp.concatenate([order, tp.astype(jnp.int32).reshape(1)])
    chunk = pl.BlockSpec((width // 2, cols), lambda *_: (0, width // cols))
    row = lambda rows, n: pl.BlockSpec((1, rows, n), lambda i, *_: (i, 0, 0))
    return pl.pallas_call(
        functools.partial(out_kernel, steps),
        grid_spec=pltpu.PrefetchScalarGridSpec(
            num_scalar_prefetch=1,
            grid=(seqs,),
            in_specs=[row(length, width)] + [chunk] * (2 * steps),
            out_specs=[row(share, steps * cols)] * tps,
        ),
        out_shape=[jax.ShapeDtypeStruct((seqs, share, steps * cols), BF16)] * tps,
        compiler_params=params(),
        cost_estimate=cost(
            2 * seqs * length * width * steps * cols,
            2 * (width * steps * cols + seqs * length * (width + steps * cols)),
        ),
        name="out_project",
    )(scalars, mixed, *[h[0] for h in held], *[h[1] for h in held])


def place_gains(me, pieces, gains):
    count, cols = len(pieces), pieces[0].shape[1]
    for i, piece in enumerate(pieces):
        at = pl.multiple_of((me + i) % count * cols, cols)
        gains[:, pl.ds(at, cols)] = piece[...]


def mid_kernel(count, me, tokens, *refs):
    parts, pieces = refs[: -3 - count], refs[-3 - count : -3]
    hidden, normed, gains = refs[-3:]
    place_gains(me[0], pieces, gains)
    total = parts[0][0].astype(F32)
    for part in parts[1:]:
        total = total + part[0].astype(F32)
    h = (
        tokens[...].astype(F32)
        + total
        * lax.rsqrt(jnp.mean(total * total, axis=-1, keepdims=True) + EPSILON)
        * gains[0:1, :]
    ).astype(BF16)
    hidden[...] = h
    v = h.astype(F32)
    normed[...] = (
        v * lax.rsqrt(jnp.mean(v * v, axis=-1, keepdims=True) + EPSILON)
    ).astype(BF16)


def mid(me, tokens, parts, gains):
    rows, width = tokens.shape
    tile = rows // 2
    row = pl.BlockSpec((tile, width), lambda i, *_: (i, 0))
    part = pl.BlockSpec((1, tile, width), lambda i, *_: (0, i, 0))
    out = jax.ShapeDtypeStruct((rows, width), BF16)
    return pl.pallas_call(
        functools.partial(mid_kernel, len(gains)),
        grid_spec=pltpu.PrefetchScalarGridSpec(
            num_scalar_prefetch=1,
            grid=(rows // tile,),
            in_specs=[row] + [part] * len(parts) + [whole_spec(g.shape) for g in gains],
            out_specs=[row, row],
            scratch_shapes=[pltpu.VMEM((2, width), F32)],
        ),
        out_shape=[out, out],
        compiler_params=params(),
        cost_estimate=cost(2e9, 2 * rows * width * (3 + len(parts))),
        name="mid",
    )(me, tokens, *parts, *gains)


def up_kernel(steps, blocks, order, scale, *refs):
    first, second = refs[:steps], refs[steps : 2 * steps]
    xs = refs[2 * steps : 2 * steps + blocks]
    out, first_full, second_full, sems = refs[2 * steps + blocks :]
    cols = first[0].shape[1]
    x = jnp.concatenate([ref[...] for ref in xs], axis=0)
    ready = [fetch(order, first, first_full, 0, cols, sems.at[0])]
    ready.append(fetch(order, second, second_full, 0, cols, sems.at[1]))
    for w, full in enumerate((first_full, second_full)):
        wait_all(ready[w])
        span = slice(w * cols, (w + 1) * cols)
        total = jnp.dot(x, full[...], preferred_element_type=F32)
        total = jnp.maximum(total * scale[:, span], 0.0)
        out[:, span] = (total * total).astype(BF16)


def up_project(order, scale, held, xs):
    steps = len(held)
    rows, width = xs[0].shape
    cols = held[0][0].shape[1]
    vmem = pl.BlockSpec(memory_space=pltpu.VMEM)
    hbm = pl.BlockSpec(memory_space=pltpu.HBM)
    return pl.pallas_call(
        functools.partial(up_kernel, steps, len(xs)),
        grid_spec=pltpu.PrefetchScalarGridSpec(
            num_scalar_prefetch=1,
            grid=(),
            in_specs=[vmem] + [hbm] * (2 * steps) + [vmem] * len(xs),
            out_specs=vmem,
            scratch_shapes=[
                pltpu.VMEM((width, cols), BF16),
                pltpu.VMEM((width, cols), BF16),
                pltpu.SemaphoreType.DMA((2, steps)),
            ],
        ),
        out_shape=jax.ShapeDtypeStruct((len(xs) * rows, 2 * cols), BF16),
        compiler_params=params(),
        cost_estimate=cost(
            4 * len(xs) * rows * width * cols,
            2 * (2 * width * cols + len(xs) * rows * (width + 2 * cols)),
        ),
        name="up_project",
    )(order, scale, *[h[0] for h in held], *[h[1] for h in held], *xs)


def down_kernel(steps, acts, *refs):
    a, chunks, outs = refs[:acts], refs[acts : acts + 2 * steps], refs[acts + 2 * steps :]
    half, cols = chunks[0].shape
    rows = outs[0].shape[1]
    for s in range(steps):
        for d, act in enumerate(a):
            total = jnp.dot(act[:, :half], chunks[2 * s][...], preferred_element_type=F32)
            total = total + jnp.dot(
                act[:, half:], chunks[2 * s + 1][...], preferred_element_type=F32
            )
            for i, out in enumerate(outs):
                out[d, :, s * cols : (s + 1) * cols] = total[i * rows : (i + 1) * rows].astype(
                    BF16
                )


def down_project(blocks, acts, held):
    rows, hidden = acts[0].shape
    rows = rows // blocks
    flat = [c for pair in held for c in pair]
    cols = flat[0].shape[1] * len(held)
    vmem = pl.BlockSpec(memory_space=pltpu.VMEM)
    return pl.pallas_call(
        functools.partial(down_kernel, len(held), len(acts)),
        in_specs=[vmem] * (len(acts) + len(flat)),
        out_specs=[vmem] * blocks,
        out_shape=[jax.ShapeDtypeStruct((len(acts), rows, cols), BF16)] * blocks,
        compiler_params=params(),
        cost_estimate=cost(
            2 * len(acts) * blocks * rows * hidden * cols,
            2 * (hidden * cols + len(acts) * blocks * rows * (hidden + cols)),
        ),
        name="down_project",
    )(*acts, *flat)


def last_kernel(streams, count, scalars, hidden, *refs):
    pieces = refs[-3 - count : -3]
    out, total, gains = refs[-3:]
    place_gains(scalars[count], pieces, gains)
    cols = hidden.shape[1] // count
    where = []
    first = 0
    for groups in streams:
        where.append([(first + g, s) for g, steps in enumerate(groups) for s in range(steps)])
        first += len(groups)
    for step in range(count):
        value = None
        for places in where:
            g, s = places[step]
            part = refs[g][0, :, s * cols : (s + 1) * cols].astype(F32)
            value = part if value is None else value + part
        to = pl.multiple_of(scalars[step] * cols, cols)
        total[:, pl.ds(to, cols)] = value
    v = total[...]
    out[...] = (
        hidden[...].astype(F32)
        + v * lax.rsqrt(jnp.mean(v * v, axis=-1, keepdims=True) + EPSILON) * gains[1:2, :]
    ).astype(BF16)


def last(scalars, hidden, streams, parts, gains):
    rows, width = hidden.shape
    tile = rows // 2
    flat = [p for stream in parts for p in stream]
    row = pl.BlockSpec((tile, width), lambda i, *_: (i, 0))
    part = lambda p: pl.BlockSpec((1, tile, p.shape[2]), lambda i, *_: (p.shape[0] - 1, i, 0))
    return pl.pallas_call(
        functools.partial(last_kernel, streams, len(gains)),
        grid_spec=pltpu.PrefetchScalarGridSpec(
            num_scalar_prefetch=1,
            grid=(rows // tile,),
            in_specs=[row] + [part(p) for p in flat] + [whole_spec(g.shape) for g in gains],
            out_specs=row,
            scratch_shapes=[pltpu.VMEM((tile, width), F32), pltpu.VMEM((2, width), F32)],
        ),
        out_shape=jax.ShapeDtypeStruct((rows, width), BF16),
        compiler_params=params(),
        cost_estimate=cost(1e9, 2 * rows * width * (2 + len(streams))),
        name="last",
    )(scalars, hidden, *flat, *gains)


def group_sizes(count):
    far = (3,) + (2,) * (count // 2 - 2) + (1,) if count > 2 else (1, 1)
    return far, (count - 1, 1)


def ring_device(
    reps,
    count,
    tps,
    tokens,
    gain_mix_pre,
    gain_mix_post,
    gain_mlp_pre,
    gain_mlp_post,
    x_weight,
    gate_weight,
    x_scale,
    gate_scale,
    conv_weight,
    recur_map,
    input_map,
    decay_param,
    out_weight,
    out_scale,
    up_weight,
    up_scale,
    down_weight,
    down_scale,
):
    rep, me, tp = (lax.axis_index(a) for a in ("rep", "fs", "tp"))
    length, width = tokens.shape[1:]
    share = length // tps
    chan = x_weight.shape[1] // reps
    hid = up_weight.shape[1] // reps

    def rep_part(value, size, axis):
        return lax.dynamic_slice_in_dim(value, rep * size, size, axis)

    pre = gain_mix_pre[:, None]
    out_mine = rep_part(out_weight, chan, 0) * out_scale
    mixer = ring_gather(
        jnp.concatenate(
            [rep_part(x_weight, chan, 1) * pre, out_mine[: chan // 2]], axis=1
        ).astype(BF16),
        jnp.concatenate(
            [rep_part(gate_weight, chan, 1) * pre, out_mine[chan // 2 :]], axis=1
        ).astype(BF16),
        count,
    )
    up_mine = (rep_part(up_weight, hid, 1) * gain_mlp_pre[:, None]).astype(BF16)
    ups = ring_gather(up_mine[:, : hid // 2], up_mine[:, hid // 2 :], count)
    down_mine = (rep_part(down_weight, hid, 0) * down_scale).astype(BF16)
    downs = ring_gather(down_mine[: hid // 2], down_mine[hid // 2 :], count)
    order = lax.dynamic_slice_in_dim(jnp.asarray(order_table(count)), me, 1, 0)[0]

    mine = lax.dynamic_slice_in_dim(tokens[0], tp * share, share, 0)
    seqs = [[tokens[0]]]
    for dr in range(1, reps):
        seqs.append([shift(mine, "rep", reps, dr)])
        for dt in range(1, tps):
            seqs[dr].append(shift(seqs[dr][0], "tp", tps, dt))
    tp_scalar = tp.astype(jnp.int32).reshape(1)
    normed_in = []
    for dr, pieces in enumerate(seqs):
        normed_in.append(normalize(tp_scalar if dr else 0 * tp_scalar, pieces))
    gains = exchange_small(jnp.stack([gain_mix_post, gain_mlp_post]), "fs", count)
    scales = jnp.concatenate([rep_part(x_scale, chan, 0), rep_part(gate_scale, chan, 0)])[None]
    same = jnp.asarray(
        (np.arange(LANES)[:, None] // BLOCK == np.arange(LANES)[None] // BLOCK), BF16
    )

    def dense_map(value):
        blocks = rep_part(value, chan, 0).reshape(chan // LANES, LANES, BLOCK)
        return jnp.tile(blocks, (1, 1, LANES // BLOCK)) * same

    maps = jnp.concatenate([dense_map(recur_map), dense_map(input_map)], axis=2)
    rate = -DECAY_SCALE * jax.nn.softplus(-rep_part(decay_param, chan, 0))[None]
    taps = rep_part(conv_weight, chan, 1)

    def over_tp(parts):
        got = [parts[0]]
        for dt in range(1, tps):
            got.append(shift(parts[dt], "tp", tps, tps - dt))
        return got

    def over_rep(summands, dr):
        total = sum(x.astype(F32) for x in summands).astype(BF16)
        return shift(total, "rep", reps, reps - dr)

    far_first = list(range(1, reps)) + [0]
    pieces = []
    for dr in far_first:
        x_branch, gate_branch = project(order, normed_in[dr], scales, mixer)
        mixed = recur(x_branch[None], gate_branch[None], taps, maps, rate)
        parts = out_project(order, tp, tps, mixed, mixer, width // count)
        summands = over_tp(parts)
        pieces += [over_rep(summands, dr)] if dr else summands
    hidden, normed = mid(me.astype(jnp.int32).reshape(1), mine, pieces, gains)

    scale = rep_part(up_scale, hid, 0)[None]
    acts = []
    for dr in range(reps):
        base = normed
        if dr:
            base = shift(normed, "rep", reps, dr)
        blocks = [base]
        for dt in range(1, tps):
            blocks.append(shift(base, "tp", tps, dt))
        acts.append(up_project(order, scale, ups, blocks))

    rows_of = {dr: [] for dr in far_first}
    for dr in far_first:
        groups = group_sizes(count)[0 if dr else 1]
        at = 0
        for steps in groups[:-1]:
            parts = down_project(tps, [acts[dr]], downs[at : at + steps])
            at += steps
            summands = over_tp(parts)
            rows_of[dr].append([over_rep(summands, dr)] if dr else summands)
    parts = down_project(tps, [acts[dr] for dr in far_first], downs[-1:])
    summands = over_tp(parts)
    for i, dr in enumerate(far_first):
        if dr:
            own = [x[i : i + 1] for x in summands]
            rows_of[dr].append([over_rep(own, dr)])
        else:
            rows_of[dr].append(summands)
    streams, arrays = [], []
    for dr in far_first:
        for i in range(len(rows_of[dr][0])):
            streams.append(group_sizes(count)[0 if dr else 1])
            arrays.append([group[i] for group in rows_of[dr]])
    scalars = jnp.concatenate([order, me.astype(jnp.int32).reshape(1)])
    return last(scalars, hidden, tuple(streams), arrays, gains)[None]


def link_states(earlier, later):
    return (earlier[0] * later[0], later[0] * earlier[1] + later[1])


def plain_device(
    tokens,
    gain_mix_pre,
    gain_mix_post,
    gain_mlp_pre,
    gain_mlp_post,
    x_weight,
    gate_weight,
    x_scale,
    gate_scale,
    conv_weight,
    recur_map,
    input_map,
    decay_param,
    out_weight,
    out_scale,
    up_weight,
    up_scale,
    down_weight,
    down_scale,
):
    resid_in = tokens[0].astype(F32)
    length = resid_in.shape[0]
    local_width = x_weight.shape[1]
    gains = lax.all_gather(
        jnp.stack(
            [gain_mix_pre, gain_mix_post, gain_mlp_pre, gain_mlp_post, out_scale, down_scale]
        ),
        "fs",
        axis=1,
        tiled=True,
    )
    gather = lambda w, axis: lax.all_gather(w.astype(BF16), "fs", axis=axis, tiled=True)
    normed = rms_rows(resid_in, gains[0]).astype(BF16)
    x_proj = jnp.dot(normed, gather(x_weight, 0), preferred_element_type=F32)
    gate_proj = jnp.dot(normed, gather(gate_weight, 0), preferred_element_type=F32)
    out_cols = gather(out_weight, 1)
    down_full = gather(down_weight, 1)
    x_branch = (x_proj * x_scale).astype(BF16)
    gate_branch = (gate_proj * gate_scale).astype(BF16)
    taps = conv_weight.shape[0]
    padded = jnp.concatenate([jnp.zeros((taps - 1, local_width), BF16), x_branch], axis=0)
    conv_sum = conv_weight[0] * padded[0:length].astype(F32)
    for k in range(1, taps):
        conv_sum = conv_sum + conv_weight[k] * padded[k : k + length].astype(F32)
    conv_out = lax.optimization_barrier(conv_sum.astype(BF16))
    blocks = local_width // BLOCK
    conv_blocks = conv_out.reshape(length, blocks, BLOCK)

    def logits(value):
        return jnp.einsum(
            "tnc,ncd->tnd",
            conv_blocks,
            value.reshape(blocks, BLOCK, BLOCK),
            preferred_element_type=F32,
        ).reshape(length, local_width)

    log_decay = (
        -DECAY_SCALE * jax.nn.sigmoid(logits(recur_map)) * jax.nn.softplus(-decay_param)
    )
    drive = (
        jnp.sqrt(-jnp.expm1(2.0 * log_decay))
        * jax.nn.sigmoid(logits(input_map))
        * conv_out.astype(F32)
    )
    _, states = lax.associative_scan(link_states, (jnp.exp(log_decay), drive), axis=0)
    mixed = (states * jax.nn.gelu(gate_branch.astype(F32))).astype(BF16)
    share_rows = length // lax.axis_size("tp")

    def scatter(left, right, scale):
        part = (jnp.dot(left, right, preferred_element_type=F32) * scale).astype(BF16)
        return lax.psum_scatter(part, "tp", scatter_dimension=0, tiled=True).astype(F32)

    mix_share = scatter(mixed, out_cols, gains[4])
    resid_share = lax.dynamic_slice_in_dim(
        resid_in, lax.axis_index("tp") * share_rows, share_rows, 0
    )
    hidden_state = (resid_share + rms_rows(mix_share, gains[1])).astype(BF16)
    normed_mlp = rms_rows(hidden_state.astype(F32), gains[2]).astype(BF16)
    mlp_input = lax.all_gather(normed_mlp, "tp", axis=0, tiled=True)
    up_proj = jnp.dot(mlp_input, gather(up_weight, 0), preferred_element_type=F32)
    activated = jnp.square(jax.nn.relu(up_proj * up_scale)).astype(BF16)
    mlp_share = scatter(activated, down_full, gains[5])
    out_share = hidden_state.astype(F32) + rms_rows(mlp_share, gains[3])
    return out_share.astype(BF16)[None]


def solution(mesh):
    in_specs = (
        P(("rep", "fs"), None, None),
        P("fs"),
        P("fs"),
        P("fs"),
        P("fs"),
        P("fs", "tp"),
        P("fs", "tp"),
        P("tp"),
        P("tp"),
        P(None, "tp"),
        P("tp", None),
        P("tp", None),
        P("tp"),
        P("tp", "fs"),
        P("fs"),
        P("fs", "tp"),
        P("tp"),
        P("tp", "fs"),
        P("fs"),
    )
    reps, count, tps = (mesh.shape[a] for a in ("rep", "fs", "tp"))

    def on_device(*args):
        tokens, x_weight, up_weight = args[0], args[5], args[15]
        (length, width), rows = tokens.shape[1:], x_weight.shape[0]
        chan, hid = x_weight.shape[1] // reps, up_weight.shape[1] // reps
        fits = (
            count % 2 == 0
            and rows % (2 * LANES) == 0
            and chan % (2 * LANES) == 0
            and chan == 2 * rows
            and chan % (width // count) == 0
            and hid % (2 * LANES) == 0
            and length % (32 * tps) == 0
            and reps * (chan // LANES) <= 8
        )
        if fits:
            return ring_device(reps, count, tps, *args)
        return plain_device(*args)

    return jax.shard_map(
        on_device,
        mesh=mesh,
        in_specs=in_specs,
        out_specs=P(("rep", "fs"), "tp", None),
        check_vma=False,
    )
```

```python
import functools

import jax
import jax.numpy as jnp
import numpy as np
from jax import lax
from jax.experimental import pallas as pl
from jax.experimental.pallas import tpu as pltpu
from jax.sharding import PartitionSpec as P


BLOCK = 32
EPSILON = 1e-06
DECAY_SCALE = 8.0
BF16 = jnp.bfloat16
F32 = jnp.float32
LANES = 128
TIME_PAD = 8
VMEM_LIMIT = 24 * 1024 * 1024


def rms_rows(values, gain_vector):
    return (
        values
        * lax.rsqrt(jnp.mean(values * values, axis=-1, keepdims=True) + EPSILON)
        * gain_vector
    )


def params(limit=VMEM_LIMIT):
    return pltpu.CompilerParams(vmem_limit_bytes=limit)


def cost(flops, bytes_accessed, transcendentals=0):
    return pl.CostEstimate(
        flops=int(flops), bytes_accessed=int(bytes_accessed), transcendentals=int(transcendentals)
    )


def whole_spec(shape):
    zeros = (0,) * len(shape)
    return pl.BlockSpec(shape, lambda *_: zeros)


def ring_order(count):
    return list(range(0, count, 2)) + [i for i in range(count - 1, 0, -1) if i % 2]


def arrival(count):
    offsets = [0]
    for k in range(1, count // 2):
        offsets += [-k, k]
    return offsets + [count // 2]


def order_table(count):
    ring = ring_order(count)
    place = {dev: i for i, dev in enumerate(ring)}
    rows = [[ring[(place[m] + off) % count] for off in arrival(count)] for m in range(count)]
    return np.asarray(rows, np.int32)


def ring_gather(first, second, count):
    ring = ring_order(count)
    fwd = [(ring[i], ring[(i + 1) % count]) for i in range(count)]
    bwd = [(b, a) for a, b in fwd]
    far = count // 2
    ahead, behind = [first, second], [first, second]
    held = [(first, second)]
    for k in range(1, far + 1):
        for h in range(2):
            if k < far or h == 0:
                ahead[h] = lax.ppermute(ahead[h], "fs", fwd)
            if k < far or h == 1:
                behind[h] = lax.ppermute(behind[h], "fs", bwd)
        if k < far:
            held += [tuple(ahead), tuple(behind)]
    return held + [(ahead[0], behind[1])]


def shift(value, axis, count, by):
    return lax.ppermute(value, axis, [((i + by) % count, i) for i in range(count)])


def exchange_small(value, axis, count):
    got = [value]
    for by in range(1, count):
        got.append(shift(value, axis, count, by))
    return got


def prepare_kernel(rep, x, gate, out, pre, scale, first, second, x_own, gate_own, out_own, sems):
    rows, cols = x_own.shape
    half = cols // 2
    wide = pl.ds(pl.multiple_of(rep[0] * cols, cols), cols)
    copies = [
        pltpu.make_async_copy(x.at[:, wide], x_own, sems.at[0]),
        pltpu.make_async_copy(gate.at[:, wide], gate_own, sems.at[1]),
        pltpu.make_async_copy(out.at[wide, :], out_own, sems.at[2]),
    ]
    for copy in copies:
        copy.start()
    gains = jnp.transpose(jnp.broadcast_to(pre[...], (LANES, rows)))
    for copy, own, to in ((copies[0], x_own, first), (copies[1], gate_own, second)):
        copy.wait()
        for at in range(0, cols, LANES):
            to[:, at : at + LANES] = (own[:, at : at + LANES] * gains).astype(BF16)
    copies[2].wait()
    first[:, cols:] = (out_own[:half, :] * scale[...]).astype(BF16)
    second[:, cols:] = (out_own[half:, :] * scale[...]).astype(BF16)


def prepare(rep, reps, x, gate, out, pre, scale):
    rows, cols = x.shape[0], x.shape[1] // reps
    shape = (rows, cols + out.shape[1])
    vmem = pl.BlockSpec(memory_space=pltpu.VMEM)
    hbm = pl.BlockSpec(memory_space=pltpu.HBM)
    return pl.pallas_call(
        prepare_kernel,
        grid_spec=pltpu.PrefetchScalarGridSpec(
            num_scalar_prefetch=1,
            grid=(),
            in_specs=[hbm] * 3 + [vmem] * 2,
            out_specs=[vmem] * 2,
            scratch_shapes=[
                pltpu.VMEM((rows, cols), F32),
                pltpu.VMEM((rows, cols), F32),
                pltpu.VMEM((cols, out.shape[1]), F32),
                pltpu.SemaphoreType.DMA((3,)),
            ],
        ),
        out_shape=[jax.ShapeDtypeStruct(shape, BF16)] * 2,
        compiler_params=params(62 * 1024 * 1024),
        cost_estimate=cost(1e6, 12 * rows * cols + 8 * rows * out.shape[1]),
        name="prepare",
    )(rep, x, gate, out, pre, scale)


def in_order(x, order, rows):
    steps = x.shape[1] // rows
    return jnp.concatenate(
        [x[:, pl.ds(pl.multiple_of(order[s] * rows, rows), rows)] for s in range(steps)], axis=1
    )


def norm_kernel(count, tp, *refs):
    out = refs[-1]
    for i in range(count):

        @pl.when(pl.program_id(0) == i)
        def _():
            v = refs[i][...].astype(F32)
            scale = lax.rsqrt(jnp.mean(v * v, axis=-1, keepdims=True) + EPSILON)
            out[...] = (v * scale).astype(BF16)


def normalize(tp, pieces):
    rows, width = pieces[0].shape
    count = len(pieces)
    return pl.pallas_call(
        functools.partial(norm_kernel, count),
        grid_spec=pltpu.PrefetchScalarGridSpec(
            num_scalar_prefetch=1,
            grid=(count,),
            in_specs=[whole_spec((rows, width))] * count,
            out_specs=pl.BlockSpec((rows, width), lambda i, tp: ((tp[0] + i) % count, 0)),
        ),
        out_shape=jax.ShapeDtypeStruct((count * rows, width), BF16),
        compiler_params=params(),
        cost_estimate=cost(1e9, 4 * count * rows * width),
        name="normalize",
    )(tp, *pieces)


def project_kernel(steps, order, normed, scale, *refs):
    outs = refs[2 * steps :]
    rows, cols = refs[0].shape[0], outs[0].shape[1]
    x = in_order(normed, order, rows)
    for h, out in enumerate(outs):
        full = jnp.concatenate([c[:, :cols] for c in refs[h * steps : (h + 1) * steps]], axis=0)
        total = jnp.dot(x, full, preferred_element_type=F32)
        out[...] = (total * scale[:, h * cols : (h + 1) * cols]).astype(BF16)


def project(order, normed, scale, held):
    steps = len(held)
    length, width = normed.shape
    cols = scale.shape[1] // 2
    out = jax.ShapeDtypeStruct((length, cols), BF16)
    vmem = pl.BlockSpec(memory_space=pltpu.VMEM)
    return pl.pallas_call(
        functools.partial(project_kernel, steps),
        grid_spec=pltpu.PrefetchScalarGridSpec(
            num_scalar_prefetch=1,
            grid=(),
            in_specs=[vmem] * (2 + 2 * steps),
            out_specs=[vmem, vmem],
        ),
        out_shape=[out, out],
        compiler_params=params(),
        cost_estimate=cost(4 * length * width * cols, 2 * (length + 2 * cols) * width),
        name="project",
    )(order, normed, scale, *[h[0] for h in held], *[h[1] for h in held])


def recur_kernel(x_ref, gate_ref, conv_ref, maps_ref, rate_ref, out_ref, pad, decay, state):
    seqs, length, width = x_ref.shape
    blocks = width // LANES
    lines = seqs * blocks
    stride = length + TIME_PAD
    taps = conv_ref.shape[0]
    pad[0:TIME_PAD, :] = jnp.zeros((TIME_PAD, LANES), F32)
    for q in range(seqs):
        for b in range(blocks):
            cols = slice(b * LANES, (b + 1) * LANES)
            base = (q * blocks + b) * stride
            pad[TIME_PAD:, :] = x_ref[q, :, cols].astype(F32)
            total = None
            for k in range(taps):
                at = TIME_PAD - (taps - 1) + k
                part = conv_ref[k : k + 1, cols] * pad[at : at + length, :]
                total = part if total is None else total + part
            conv = total.astype(BF16)
            logits = jnp.dot(conv, maps_ref[b], preferred_element_type=F32)
            log_decay = rate_ref[:, cols] * jax.nn.sigmoid(logits[:, :LANES])
            a = jnp.exp(log_decay)
            y = 2.0 * log_decay
            series = -y * (
                1.0
                + y * (1 / 2 + y * (1 / 6 + y * (1 / 24 + y * (1 / 120 + y * (1 / 720)))))
            )
            loss = jnp.where(y > -0.4, series, 1.0 - a * a)
            decay[base : base + length, :] = a
            state[base : base + length, :] = (
                jnp.sqrt(loss) * jax.nn.sigmoid(logits[:, LANES:]) * conv.astype(F32)
            )

    def advance(t, h):
        at = pl.ds(t, lines, stride=stride)
        h = decay[at, :] * h + state[at, :]
        state[at, :] = h
        return h

    lax.fori_loop(0, length, advance, jnp.zeros((lines, LANES), F32), unroll=16)
    for q in range(seqs):
        for b in range(blocks):
            cols = slice(b * LANES, (b + 1) * LANES)
            base = (q * blocks + b) * stride
            g = gate_ref[q, :, cols].astype(F32)
            out_ref[q, :, cols] = (
                state[base : base + length, :] * jax.nn.gelu(g)
            ).astype(BF16)


def recur(x_branch, gate_branch, conv_weight, maps, rate):
    seqs, length, width = x_branch.shape
    lines = seqs * (width // LANES)
    rows = lines * (length + TIME_PAD)
    vmem = pl.BlockSpec(memory_space=pltpu.VMEM)
    return pl.pallas_call(
        recur_kernel,
        in_specs=[vmem] * 5,
        out_specs=vmem,
        out_shape=jax.ShapeDtypeStruct(x_branch.shape, BF16),
        scratch_shapes=[
            pltpu.VMEM((length + TIME_PAD, LANES), F32),
            pltpu.VMEM((rows, LANES), F32),
            pltpu.VMEM((rows, LANES), F32),
        ],
        compiler_params=params(),
        cost_estimate=cost(3e9, 6 * x_branch.size, 10 * x_branch.size),
        name="recur",
    )(x_branch, gate_branch, conv_weight, maps, rate)


def out_kernel(steps, cols, order, mixed, *refs):
    top, low = refs[:steps], refs[steps : 2 * steps]
    outs = refs[2 * steps :]
    tps, share = len(outs), outs[0].shape[1]
    half = top[0].shape[0]
    pieces = []
    for j in range(tps):
        at = pl.multiple_of((order[steps] + j) % tps * share, share)
        pieces.append(mixed[0, pl.ds(at, share), :])
    m = jnp.concatenate(pieces, axis=0)
    for s in range(steps):
        at = pl.multiple_of(order[s] * cols, cols)
        part = jnp.dot(m[:, :half], top[s][:, -cols:], preferred_element_type=F32)
        part = part + jnp.dot(m[:, half:], low[s][:, -cols:], preferred_element_type=F32)
        for j, out in enumerate(outs):
            out[0, :, pl.ds(at, cols)] = part[j * share : (j + 1) * share].astype(BF16)


def out_project(order, tp, tps, mixed, held, cols):
    steps = len(held)
    _, length, width = mixed.shape
    share = length // tps
    scalars = jnp.concatenate([order, tp])
    vmem = pl.BlockSpec(memory_space=pltpu.VMEM)
    return pl.pallas_call(
        functools.partial(out_kernel, steps, cols),
        grid_spec=pltpu.PrefetchScalarGridSpec(
            num_scalar_prefetch=1,
            grid=(),
            in_specs=[vmem] * (1 + 2 * steps),
            out_specs=[vmem] * tps,
        ),
        out_shape=[jax.ShapeDtypeStruct((1, share, steps * cols), BF16)] * tps,
        compiler_params=params(),
        cost_estimate=cost(
            2 * length * width * steps * cols,
            2 * (width * steps * cols + length * (width + steps * cols)),
        ),
        name="out_project",
    )(scalars, mixed, *[h[0] for h in held], *[h[1] for h in held])


def place_gains(me, pieces, gains):
    count, cols = len(pieces), pieces[0].shape[1]
    for i, piece in enumerate(pieces):
        at = pl.multiple_of((me + i) % count * cols, cols)
        gains[:, pl.ds(at, cols)] = piece[...]


def mid_kernel(count, me, tokens, *refs):
    parts, pieces = refs[: -3 - count], refs[-3 - count : -3]
    hidden, normed, gains = refs[-3:]
    place_gains(me[0], pieces, gains)
    total = parts[0][0].astype(F32)
    for part in parts[1:]:
        total = total + part[0].astype(F32)
    h = (
        tokens[...].astype(F32)
        + total
        * lax.rsqrt(jnp.mean(total * total, axis=-1, keepdims=True) + EPSILON)
        * gains[0:1, :]
    ).astype(BF16)
    hidden[...] = h
    v = h.astype(F32)
    normed[...] = (
        v * lax.rsqrt(jnp.mean(v * v, axis=-1, keepdims=True) + EPSILON)
    ).astype(BF16)


def mid(me, tokens, parts, gains):
    rows, width = tokens.shape
    tile = rows // 2
    row = pl.BlockSpec((tile, width), lambda i, *_: (i, 0))
    part = pl.BlockSpec((1, tile, width), lambda i, *_: (0, i, 0))
    out = jax.ShapeDtypeStruct((rows, width), BF16)
    return pl.pallas_call(
        functools.partial(mid_kernel, len(gains)),
        grid_spec=pltpu.PrefetchScalarGridSpec(
            num_scalar_prefetch=1,
            grid=(rows // tile,),
            in_specs=[row] + [part] * len(parts) + [whole_spec(g.shape) for g in gains],
            out_specs=[row, row],
            scratch_shapes=[pltpu.VMEM((2, width), F32)],
        ),
        out_shape=[out, out],
        compiler_params=params(),
        cost_estimate=cost(2e9, 2 * rows * width * (3 + len(parts))),
        name="mid",
    )(me, tokens, *parts, *gains)


def up_kernel(steps, blocks, order, scale, *refs):
    xs = refs[2 * steps : 2 * steps + blocks]
    out = refs[-1]
    rows, cols = refs[0].shape
    x = jnp.concatenate([in_order(ref, order, rows) for ref in xs], axis=0)
    for h in range(2):
        full = jnp.concatenate([c[...] for c in refs[h * steps : (h + 1) * steps]], axis=0)
        span = slice(h * cols, (h + 1) * cols)
        total = jnp.dot(x, full, preferred_element_type=F32)
        total = jnp.maximum(total * scale[:, span], 0.0)
        out[:, span] = (total * total).astype(BF16)


def up_project(order, scale, held, xs):
    steps = len(held)
    rows, width = xs[0].shape
    cols = held[0][0].shape[1]
    vmem = pl.BlockSpec(memory_space=pltpu.VMEM)
    return pl.pallas_call(
        functools.partial(up_kernel, steps, len(xs)),
        grid_spec=pltpu.PrefetchScalarGridSpec(
            num_scalar_prefetch=1,
            grid=(),
            in_specs=[vmem] * (1 + 2 * steps + len(xs)),
            out_specs=vmem,
        ),
        out_shape=jax.ShapeDtypeStruct((len(xs) * rows, 2 * cols), BF16),
        compiler_params=params(),
        cost_estimate=cost(
            4 * len(xs) * rows * width * cols,
            2 * (2 * width * cols + len(xs) * rows * (width + 2 * cols)),
        ),
        name="up_project",
    )(order, scale, *[h[0] for h in held], *[h[1] for h in held], *xs)


def down_kernel(steps, acts, *refs):
    a, chunks, outs = refs[:acts], refs[acts : acts + 2 * steps], refs[acts + 2 * steps :]
    half, cols = chunks[0].shape
    rows = outs[0].shape[1]
    for s in range(steps):
        for d, act in enumerate(a):
            total = jnp.dot(act[:, :half], chunks[2 * s][...], preferred_element_type=F32)
            total = total + jnp.dot(
                act[:, half:], chunks[2 * s + 1][...], preferred_element_type=F32
            )
            for i, out in enumerate(outs):
                out[d, :, s * cols : (s + 1) * cols] = total[i * rows : (i + 1) * rows].astype(
                    BF16
                )


def down_project(blocks, acts, held):
    rows, hidden = acts[0].shape
    rows = rows // blocks
    flat = [c for pair in held for c in pair]
    cols = flat[0].shape[1] * len(held)
    vmem = pl.BlockSpec(memory_space=pltpu.VMEM)
    return pl.pallas_call(
        functools.partial(down_kernel, len(held), len(acts)),
        in_specs=[vmem] * (len(acts) + len(flat)),
        out_specs=[vmem] * blocks,
        out_shape=[jax.ShapeDtypeStruct((len(acts), rows, cols), BF16)] * blocks,
        compiler_params=params(),
        cost_estimate=cost(
            2 * len(acts) * blocks * rows * hidden * cols,
            2 * (hidden * cols + len(acts) * blocks * rows * (hidden + cols)),
        ),
        name="down_project",
    )(*acts, *flat)


def last_kernel(streams, count, scalars, hidden, *refs):
    pieces = refs[-3 - count : -3]
    out, total, gains = refs[-3:]
    place_gains(scalars[count], pieces, gains)
    cols = hidden.shape[1] // count
    where = []
    first = 0
    for groups in streams:
        where.append([(first + g, s) for g, steps in enumerate(groups) for s in range(steps)])
        first += len(groups)
    for step in range(count):
        value = None
        for places in where:
            g, s = places[step]
            part = refs[g][0, :, s * cols : (s + 1) * cols].astype(F32)
            value = part if value is None else value + part
        to = pl.multiple_of(scalars[step] * cols, cols)
        total[:, pl.ds(to, cols)] = value
    v = total[...]
    out[...] = (
        hidden[...].astype(F32)
        + v * lax.rsqrt(jnp.mean(v * v, axis=-1, keepdims=True) + EPSILON) * gains[1:2, :]
    ).astype(BF16)


def last(scalars, hidden, streams, parts, gains):
    rows, width = hidden.shape
    tile = rows // 2
    flat = [p for stream in parts for p in stream]
    row = pl.BlockSpec((tile, width), lambda i, *_: (i, 0))
    part = lambda p: pl.BlockSpec((1, tile, p.shape[2]), lambda i, *_: (p.shape[0] - 1, i, 0))
    return pl.pallas_call(
        functools.partial(last_kernel, streams, len(gains)),
        grid_spec=pltpu.PrefetchScalarGridSpec(
            num_scalar_prefetch=1,
            grid=(rows // tile,),
            in_specs=[row] + [part(p) for p in flat] + [whole_spec(g.shape) for g in gains],
            out_specs=row,
            scratch_shapes=[pltpu.VMEM((tile, width), F32), pltpu.VMEM((2, width), F32)],
        ),
        out_shape=jax.ShapeDtypeStruct((rows, width), BF16),
        compiler_params=params(),
        cost_estimate=cost(1e9, 2 * rows * width * (2 + len(streams))),
        name="last",
    )(scalars, hidden, *flat, *gains)


def group_sizes(count):
    far = (3,) + (2,) * (count // 2 - 2) + (1,) if count > 2 else (1, 1)
    return far, (count - 1, 1)


def ring_device(
    reps,
    count,
    tps,
    tokens,
    gain_mix_pre,
    gain_mix_post,
    gain_mlp_pre,
    gain_mlp_post,
    x_weight,
    gate_weight,
    x_scale,
    gate_scale,
    conv_weight,
    recur_map,
    input_map,
    decay_param,
    out_weight,
    out_scale,
    up_weight,
    up_scale,
    down_weight,
    down_scale,
):
    rep, me, tp = (lax.axis_index(a) for a in ("rep", "fs", "tp"))
    length, width = tokens.shape[1:]
    share = length // tps
    chan = x_weight.shape[1] // reps
    hid = up_weight.shape[1] // reps

    def rep_part(value, size, axis):
        return lax.dynamic_slice_in_dim(value, rep * size, size, axis)

    rep_scalar, tp_scalar, me_scalar = (i.astype(jnp.int32).reshape(1) for i in (rep, tp, me))
    halves = prepare(
        rep_scalar, reps, x_weight, gate_weight, out_weight, gain_mix_pre[None], out_scale[None]
    )
    mixer = ring_gather(*halves, count)
    up_mine = (rep_part(up_weight, hid, 1) * gain_mlp_pre[:, None]).astype(BF16)
    ups = ring_gather(up_mine[:, : hid // 2], up_mine[:, hid // 2 :], count)
    down_mine = (rep_part(down_weight, hid, 0) * down_scale).astype(BF16)
    downs = ring_gather(down_mine[: hid // 2], down_mine[hid // 2 :], count)
    order = lax.dynamic_slice_in_dim(jnp.asarray(order_table(count)), me, 1, 0)[0]

    mine = lax.dynamic_slice_in_dim(tokens[0], tp * share, share, 0)
    seqs = [[tokens[0]]]
    for dr in range(1, reps):
        seqs.append([shift(mine, "rep", reps, dr)])
        for dt in range(1, tps):
            seqs[dr].append(shift(seqs[dr][0], "tp", tps, dt))
    normed_in = []
    for dr, pieces in enumerate(seqs):
        normed_in.append(normalize(tp_scalar if dr else 0 * tp_scalar, pieces))
    gains = exchange_small(jnp.stack([gain_mix_post, gain_mlp_post]), "fs", count)
    scales = jnp.concatenate([rep_part(x_scale, chan, 0), rep_part(gate_scale, chan, 0)])[None]
    same = jnp.asarray(
        (np.arange(LANES)[:, None] // BLOCK == np.arange(LANES)[None] // BLOCK), BF16
    )

    def dense_map(value):
        blocks = rep_part(value, chan, 0).reshape(chan // LANES, LANES, BLOCK)
        return jnp.tile(blocks, (1, 1, LANES // BLOCK)) * same

    maps = jnp.concatenate([dense_map(recur_map), dense_map(input_map)], axis=2)
    rate = -DECAY_SCALE * jax.nn.softplus(-rep_part(decay_param, chan, 0))[None]
    taps = rep_part(conv_weight, chan, 1)

    def over_tp(parts):
        got = [parts[0]]
        for dt in range(1, tps):
            got.append(shift(parts[dt], "tp", tps, tps - dt))
        return got

    def over_rep(summands, dr):
        total = sum(x.astype(F32) for x in summands).astype(BF16)
        return shift(total, "rep", reps, reps - dr)

    far_first = list(range(1, reps)) + [0]
    pieces = []
    for dr in far_first:
        x_branch, gate_branch = project(order, normed_in[dr], scales, mixer)
        mixed = recur(x_branch[None], gate_branch[None], taps, maps, rate)
        parts = out_project(order, tp_scalar, tps, mixed, mixer, width // count)
        summands = over_tp(parts)
        pieces += [over_rep(summands, dr)] if dr else summands
    hidden, normed = mid(me_scalar, mine, pieces, gains)

    scale = rep_part(up_scale, hid, 0)[None]
    acts = []
    for dr in range(reps):
        base = normed
        if dr:
            base = shift(normed, "rep", reps, dr)
        blocks = [base]
        for dt in range(1, tps):
            blocks.append(shift(base, "tp", tps, dt))
        acts.append(up_project(order, scale, ups, blocks))

    rows_of = {dr: [] for dr in far_first}
    for dr in far_first:
        groups = group_sizes(count)[0 if dr else 1]
        at = 0
        for steps in groups[:-1]:
            parts = down_project(tps, [acts[dr]], downs[at : at + steps])
            at += steps
            summands = over_tp(parts)
            rows_of[dr].append([over_rep(summands, dr)] if dr else summands)
    parts = down_project(tps, [acts[dr] for dr in far_first], downs[-1:])
    summands = over_tp(parts)
    for i, dr in enumerate(far_first):
        if dr:
            own = [x[i : i + 1] for x in summands]
            rows_of[dr].append([over_rep(own, dr)])
        else:
            rows_of[dr].append(summands)
    streams, arrays = [], []
    for dr in far_first:
        for i in range(len(rows_of[dr][0])):
            streams.append(group_sizes(count)[0 if dr else 1])
            arrays.append([group[i] for group in rows_of[dr]])
    scalars = jnp.concatenate([order, me_scalar])
    return last(scalars, hidden, tuple(streams), arrays, gains)[None]


def link_states(earlier, later):
    return (earlier[0] * later[0], later[0] * earlier[1] + later[1])


def plain_device(
    tokens,
    gain_mix_pre,
    gain_mix_post,
    gain_mlp_pre,
    gain_mlp_post,
    x_weight,
    gate_weight,
    x_scale,
    gate_scale,
    conv_weight,
    recur_map,
    input_map,
    decay_param,
    out_weight,
    out_scale,
    up_weight,
    up_scale,
    down_weight,
    down_scale,
):
    resid_in = tokens[0].astype(F32)
    length = resid_in.shape[0]
    local_width = x_weight.shape[1]
    gains = lax.all_gather(
        jnp.stack(
            [gain_mix_pre, gain_mix_post, gain_mlp_pre, gain_mlp_post, out_scale, down_scale]
        ),
        "fs",
        axis=1,
        tiled=True,
    )
    gather = lambda w, axis: lax.all_gather(w.astype(BF16), "fs", axis=axis, tiled=True)
    normed = rms_rows(resid_in, gains[0]).astype(BF16)
    x_proj = jnp.dot(normed, gather(x_weight, 0), preferred_element_type=F32)
    gate_proj = jnp.dot(normed, gather(gate_weight, 0), preferred_element_type=F32)
    out_cols = gather(out_weight, 1)
    down_full = gather(down_weight, 1)
    x_branch = (x_proj * x_scale).astype(BF16)
    gate_branch = (gate_proj * gate_scale).astype(BF16)
    taps = conv_weight.shape[0]
    padded = jnp.concatenate([jnp.zeros((taps - 1, local_width), BF16), x_branch], axis=0)
    conv_sum = conv_weight[0] * padded[0:length].astype(F32)
    for k in range(1, taps):
        conv_sum = conv_sum + conv_weight[k] * padded[k : k + length].astype(F32)
    conv_out = lax.optimization_barrier(conv_sum.astype(BF16))
    blocks = local_width // BLOCK
    conv_blocks = conv_out.reshape(length, blocks, BLOCK)

    def logits(value):
        return jnp.einsum(
            "tnc,ncd->tnd",
            conv_blocks,
            value.reshape(blocks, BLOCK, BLOCK),
            preferred_element_type=F32,
        ).reshape(length, local_width)

    log_decay = (
        -DECAY_SCALE * jax.nn.sigmoid(logits(recur_map)) * jax.nn.softplus(-decay_param)
    )
    drive = (
        jnp.sqrt(-jnp.expm1(2.0 * log_decay))
        * jax.nn.sigmoid(logits(input_map))
        * conv_out.astype(F32)
    )
    _, states = lax.associative_scan(link_states, (jnp.exp(log_decay), drive), axis=0)
    mixed = (states * jax.nn.gelu(gate_branch.astype(F32))).astype(BF16)
    share_rows = length // lax.axis_size("tp")

    def scatter(left, right, scale):
        part = (jnp.dot(left, right, preferred_element_type=F32) * scale).astype(BF16)
        return lax.psum_scatter(part, "tp", scatter_dimension=0, tiled=True).astype(F32)

    mix_share = scatter(mixed, out_cols, gains[4])
    resid_share = lax.dynamic_slice_in_dim(
        resid_in, lax.axis_index("tp") * share_rows, share_rows, 0
    )
    hidden_state = (resid_share + rms_rows(mix_share, gains[1])).astype(BF16)
    normed_mlp = rms_rows(hidden_state.astype(F32), gains[2]).astype(BF16)
    mlp_input = lax.all_gather(normed_mlp, "tp", axis=0, tiled=True)
    up_proj = jnp.dot(mlp_input, gather(up_weight, 0), preferred_element_type=F32)
    activated = jnp.square(jax.nn.relu(up_proj * up_scale)).astype(BF16)
    mlp_share = scatter(activated, down_full, gains[5])
    out_share = hidden_state.astype(F32) + rms_rows(mlp_share, gains[3])
    return out_share.astype(BF16)[None]


def solution(mesh):
    in_specs = (
        P(("rep", "fs"), None, None),
        P("fs"),
        P("fs"),
        P("fs"),
        P("fs"),
        P("fs", "tp"),
        P("fs", "tp"),
        P("tp"),
        P("tp"),
        P(None, "tp"),
        P("tp", None),
        P("tp", None),
        P("tp"),
        P("tp", "fs"),
        P("fs"),
        P("fs", "tp"),
        P("tp"),
        P("tp", "fs"),
        P("fs"),
    )
    reps, count, tps = (mesh.shape[a] for a in ("rep", "fs", "tp"))

    def on_device(*args):
        tokens, x_weight, up_weight = args[0], args[5], args[15]
        (length, width), rows = tokens.shape[1:], x_weight.shape[0]
        chan, hid = x_weight.shape[1] // reps, up_weight.shape[1] // reps
        fits = (
            count % 2 == 0
            and rows % (2 * LANES) == 0
            and chan % (2 * LANES) == 0
            and chan == 2 * rows
            and chan % (width // count) == 0
            and hid % (2 * LANES) == 0
            and length % (32 * tps) == 0
            and reps * (chan // LANES) <= 8
        )
        if fits:
            return ring_device(reps, count, tps, *args)
        return plain_device(*args)

    return jax.shard_map(
        on_device,
        mesh=mesh,
        in_specs=in_specs,
        out_specs=P(("rep", "fs"), "tp", None),
        check_vma=False,
    )
```

```python
import functools

import jax
import jax.numpy as jnp
import numpy as np
from jax import lax
from jax.experimental import pallas as pl
from jax.experimental.pallas import tpu as pltpu
from jax.sharding import PartitionSpec as P


BLOCK = 32
EPSILON = 1e-06
DECAY_SCALE = 8.0
BF16 = jnp.bfloat16
F32 = jnp.float32
LANES = 128
TIME_PAD = 8
VMEM_LIMIT = 24 * 1024 * 1024


def rms_rows(values, gain_vector):
    return (
        values
        * lax.rsqrt(jnp.mean(values * values, axis=-1, keepdims=True) + EPSILON)
        * gain_vector
    )


def params(limit=VMEM_LIMIT):
    return pltpu.CompilerParams(vmem_limit_bytes=limit)


def cost(flops, bytes_accessed, transcendentals=0):
    return pl.CostEstimate(
        flops=int(flops), bytes_accessed=int(bytes_accessed), transcendentals=int(transcendentals)
    )


def whole_spec(shape):
    zeros = (0,) * len(shape)
    return pl.BlockSpec(shape, lambda *_: zeros)


def ring_order(count):
    return list(range(0, count, 2)) + [i for i in range(count - 1, 0, -1) if i % 2]


def arrival(count):
    offsets = [0]
    for k in range(1, count // 2):
        offsets += [-k, k]
    return offsets + [count // 2]


def order_table(count):
    ring = ring_order(count)
    place = {dev: i for i, dev in enumerate(ring)}
    rows = [[ring[(place[m] + off) % count] for off in arrival(count)] for m in range(count)]
    return np.asarray(rows, np.int32)


def ring_gather(first, second, count):
    ring = ring_order(count)
    fwd = [(ring[i], ring[(i + 1) % count]) for i in range(count)]
    bwd = [(b, a) for a, b in fwd]
    far = count // 2
    ahead, behind = [first, second], [first, second]
    held = [(first, second)]
    for k in range(1, far + 1):
        for h in range(2):
            if k < far or h == 0:
                ahead[h] = lax.ppermute(ahead[h], "fs", fwd)
            if k < far or h == 1:
                behind[h] = lax.ppermute(behind[h], "fs", bwd)
        if k < far:
            held += [tuple(ahead), tuple(behind)]
    return held + [(ahead[0], behind[1])]


def shift(value, axis, count, by):
    return lax.ppermute(value, axis, [((i + by) % count, i) for i in range(count)])


def exchange_small(value, axis, count):
    got = [value]
    for by in range(1, count):
        got.append(shift(value, axis, count, by))
    return got


def prepare_kernel(rep, x, gate, out, pre_all, scale_all, first, second, *scratch):
    x_own, gate_own, out_own, pre, scale, sems = scratch
    rows, cols = x_own.shape
    half = cols // 2
    wide = pl.ds(pl.multiple_of(rep[0] * cols, cols), cols)
    copies = [
        pltpu.make_async_copy(x.at[:, wide], x_own, sems.at[0]),
        pltpu.make_async_copy(gate.at[:, wide], gate_own, sems.at[1]),
        pltpu.make_async_copy(out.at[wide, :], out_own, sems.at[2]),
        pltpu.make_async_copy(pre_all, pre, sems.at[3]),
        pltpu.make_async_copy(scale_all, scale, sems.at[4]),
    ]
    for copy in copies:
        copy.start()
    copies[3].wait()
    gains = jnp.transpose(jnp.broadcast_to(pre[...], (LANES, rows)))
    for copy, own, to in ((copies[0], x_own, first), (copies[1], gate_own, second)):
        copy.wait()
        for at in range(0, cols, LANES):
            to[:, at : at + LANES] = (own[:, at : at + LANES] * gains).astype(BF16)
    copies[2].wait()
    copies[4].wait()
    first[:, cols:] = (out_own[:half, :] * scale[...]).astype(BF16)
    second[:, cols:] = (out_own[half:, :] * scale[...]).astype(BF16)


def prepare(rep, reps, x, gate, out, pre, scale):
    rows, cols = x.shape[0], x.shape[1] // reps
    shape = (rows, cols + out.shape[1])
    vmem = pl.BlockSpec(memory_space=pltpu.VMEM)
    hbm = pl.BlockSpec(memory_space=pltpu.HBM)
    return pl.pallas_call(
        prepare_kernel,
        grid_spec=pltpu.PrefetchScalarGridSpec(
            num_scalar_prefetch=1,
            grid=(),
            in_specs=[hbm] * 5,
            out_specs=[vmem] * 2,
            scratch_shapes=[
                pltpu.VMEM((rows, cols), F32),
                pltpu.VMEM((rows, cols), F32),
                pltpu.VMEM((cols, out.shape[1]), F32),
                pltpu.VMEM(pre.shape, F32),
                pltpu.VMEM(scale.shape, F32),
                pltpu.SemaphoreType.DMA((5,)),
            ],
        ),
        out_shape=[jax.ShapeDtypeStruct(shape, BF16)] * 2,
        compiler_params=params(62 * 1024 * 1024),
        cost_estimate=cost(1e6, 12 * rows * cols + 8 * rows * out.shape[1]),
        name="prepare",
    )(rep, x, gate, out, pre, scale)


def in_order(x, order, rows):
    steps = x.shape[1] // rows
    return jnp.concatenate(
        [x[:, pl.ds(pl.multiple_of(order[s] * rows, rows), rows)] for s in range(steps)], axis=1
    )


def norm_kernel(count, tp, *refs):
    out = refs[-1]
    for i in range(count):

        @pl.when(pl.program_id(0) == i)
        def _():
            v = refs[i][...].astype(F32)
            scale = lax.rsqrt(jnp.mean(v * v, axis=-1, keepdims=True) + EPSILON)
            out[...] = (v * scale).astype(BF16)


def normalize(tp, pieces):
    rows, width = pieces[0].shape
    count = len(pieces)
    return pl.pallas_call(
        functools.partial(norm_kernel, count),
        grid_spec=pltpu.PrefetchScalarGridSpec(
            num_scalar_prefetch=1,
            grid=(count,),
            in_specs=[whole_spec((rows, width))] * count,
            out_specs=pl.BlockSpec((rows, width), lambda i, tp: ((tp[0] + i) % count, 0)),
        ),
        out_shape=jax.ShapeDtypeStruct((count * rows, width), BF16),
        compiler_params=params(),
        cost_estimate=cost(1e9, 4 * count * rows * width),
        name="normalize",
    )(tp, *pieces)


def project_kernel(steps, order, normed, scale, *refs):
    outs = refs[2 * steps :]
    rows, cols = refs[0].shape[0], outs[0].shape[1]
    x = in_order(normed, order, rows)
    for h, out in enumerate(outs):
        full = jnp.concatenate([c[:, :cols] for c in refs[h * steps : (h + 1) * steps]], axis=0)
        total = jnp.dot(x, full, preferred_element_type=F32)
        out[...] = (total * scale[:, h * cols : (h + 1) * cols]).astype(BF16)


def project(order, normed, scale, held):
    steps = len(held)
    length, width = normed.shape
    cols = scale.shape[1] // 2
    out = jax.ShapeDtypeStruct((length, cols), BF16)
    vmem = pl.BlockSpec(memory_space=pltpu.VMEM)
    return pl.pallas_call(
        functools.partial(project_kernel, steps),
        grid_spec=pltpu.PrefetchScalarGridSpec(
            num_scalar_prefetch=1,
            grid=(),
            in_specs=[vmem] * (2 + 2 * steps),
            out_specs=[vmem, vmem],
        ),
        out_shape=[out, out],
        compiler_params=params(),
        cost_estimate=cost(4 * length * width * cols, 2 * (length + 2 * cols) * width),
        name="project",
    )(order, normed, scale, *[h[0] for h in held], *[h[1] for h in held])


def recur_kernel(x_ref, gate_ref, conv_ref, maps_ref, rate_ref, out_ref, pad, decay, state):
    seqs, length, width = x_ref.shape
    blocks = width // LANES
    lines = seqs * blocks
    stride = length + TIME_PAD
    taps = conv_ref.shape[0]
    pad[0:TIME_PAD, :] = jnp.zeros((TIME_PAD, LANES), F32)
    for q in range(seqs):
        for b in range(blocks):
            cols = slice(b * LANES, (b + 1) * LANES)
            base = (q * blocks + b) * stride
            pad[TIME_PAD:, :] = x_ref[q, :, cols].astype(F32)
            total = None
            for k in range(taps):
                at = TIME_PAD - (taps - 1) + k
                part = conv_ref[k : k + 1, cols] * pad[at : at + length, :]
                total = part if total is None else total + part
            conv = total.astype(BF16)
            logits = jnp.dot(conv, maps_ref[b], preferred_element_type=F32)
            log_decay = rate_ref[:, cols] * jax.nn.sigmoid(logits[:, :LANES])
            a = jnp.exp(log_decay)
            y = 2.0 * log_decay
            series = -y * (
                1.0
                + y * (1 / 2 + y * (1 / 6 + y * (1 / 24 + y * (1 / 120 + y * (1 / 720)))))
            )
            loss = jnp.where(y > -0.4, series, 1.0 - a * a)
            decay[base : base + length, :] = a
            state[base : base + length, :] = (
                jnp.sqrt(loss) * jax.nn.sigmoid(logits[:, LANES:]) * conv.astype(F32)
            )

    def advance(t, h):
        at = pl.ds(t, lines, stride=stride)
        h = decay[at, :] * h + state[at, :]
        state[at, :] = h
        return h

    lax.fori_loop(0, length, advance, jnp.zeros((lines, LANES), F32), unroll=16)
    for q in range(seqs):
        for b in range(blocks):
            cols = slice(b * LANES, (b + 1) * LANES)
            base = (q * blocks + b) * stride
            g = gate_ref[q, :, cols].astype(F32)
            out_ref[q, :, cols] = (
                state[base : base + length, :] * jax.nn.gelu(g)
            ).astype(BF16)


def recur(x_branch, gate_branch, conv_weight, maps, rate):
    seqs, length, width = x_branch.shape
    lines = seqs * (width // LANES)
    rows = lines * (length + TIME_PAD)
    vmem = pl.BlockSpec(memory_space=pltpu.VMEM)
    return pl.pallas_call(
        recur_kernel,
        in_specs=[vmem] * 5,
        out_specs=vmem,
        out_shape=jax.ShapeDtypeStruct(x_branch.shape, BF16),
        scratch_shapes=[
            pltpu.VMEM((length + TIME_PAD, LANES), F32),
            pltpu.VMEM((rows, LANES), F32),
            pltpu.VMEM((rows, LANES), F32),
        ],
        compiler_params=params(),
        cost_estimate=cost(3e9, 6 * x_branch.size, 10 * x_branch.size),
        name="recur",
    )(x_branch, gate_branch, conv_weight, maps, rate)


def out_kernel(steps, cols, order, mixed, *refs):
    top, low = refs[:steps], refs[steps : 2 * steps]
    outs = refs[2 * steps :]
    tps, share = len(outs), outs[0].shape[1]
    half = top[0].shape[0]
    pieces = []
    for j in range(tps):
        at = pl.multiple_of((order[steps] + j) % tps * share, share)
        pieces.append(mixed[0, pl.ds(at, share), :])
    m = jnp.concatenate(pieces, axis=0)
    for s in range(steps):
        at = pl.multiple_of(order[s] * cols, cols)
        part = jnp.dot(m[:, :half], top[s][:, -cols:], preferred_element_type=F32)
        part = part + jnp.dot(m[:, half:], low[s][:, -cols:], preferred_element_type=F32)
        for j, out in enumerate(outs):
            out[0, :, pl.ds(at, cols)] = part[j * share : (j + 1) * share].astype(BF16)


def out_project(order, tp, tps, mixed, held, cols):
    steps = len(held)
    _, length, width = mixed.shape
    share = length // tps
    scalars = jnp.concatenate([order, tp])
    vmem = pl.BlockSpec(memory_space=pltpu.VMEM)
    return pl.pallas_call(
        functools.partial(out_kernel, steps, cols),
        grid_spec=pltpu.PrefetchScalarGridSpec(
            num_scalar_prefetch=1,
            grid=(),
            in_specs=[vmem] * (1 + 2 * steps),
            out_specs=[vmem] * tps,
        ),
        out_shape=[jax.ShapeDtypeStruct((1, share, steps * cols), BF16)] * tps,
        compiler_params=params(),
        cost_estimate=cost(
            2 * length * width * steps * cols,
            2 * (width * steps * cols + length * (width + steps * cols)),
        ),
        name="out_project",
    )(scalars, mixed, *[h[0] for h in held], *[h[1] for h in held])


def place_gains(me, pieces, gains):
    count, cols = len(pieces), pieces[0].shape[1]
    for i, piece in enumerate(pieces):
        at = pl.multiple_of((me + i) % count * cols, cols)
        gains[:, pl.ds(at, cols)] = piece[...]


def mid_kernel(count, me, tokens, *refs):
    parts, pieces = refs[: -3 - count], refs[-3 - count : -3]
    hidden, normed, gains = refs[-3:]
    place_gains(me[0], pieces, gains)
    total = parts[0][0].astype(F32)
    for part in parts[1:]:
        total = total + part[0].astype(F32)
    h = (
        tokens[...].astype(F32)
        + total
        * lax.rsqrt(jnp.mean(total * total, axis=-1, keepdims=True) + EPSILON)
        * gains[0:1, :]
    ).astype(BF16)
    hidden[...] = h
    v = h.astype(F32)
    normed[...] = (
        v * lax.rsqrt(jnp.mean(v * v, axis=-1, keepdims=True) + EPSILON)
    ).astype(BF16)


def mid(me, tokens, parts, gains):
    rows, width = tokens.shape
    tile = rows // 2
    row = pl.BlockSpec((tile, width), lambda i, *_: (i, 0))
    part = pl.BlockSpec((1, tile, width), lambda i, *_: (0, i, 0))
    out = jax.ShapeDtypeStruct((rows, width), BF16)
    return pl.pallas_call(
        functools.partial(mid_kernel, len(gains)),
        grid_spec=pltpu.PrefetchScalarGridSpec(
            num_scalar_prefetch=1,
            grid=(rows // tile,),
            in_specs=[row] + [part] * len(parts) + [whole_spec(g.shape) for g in gains],
            out_specs=[row, row],
            scratch_shapes=[pltpu.VMEM((2, width), F32)],
        ),
        out_shape=[out, out],
        compiler_params=params(),
        cost_estimate=cost(2e9, 2 * rows * width * (3 + len(parts))),
        name="mid",
    )(me, tokens, *parts, *gains)


def up_kernel(steps, blocks, order, scale, *refs):
    xs = refs[2 * steps : 2 * steps + blocks]
    out = refs[-1]
    rows, cols = refs[0].shape
    x = jnp.concatenate([in_order(ref, order, rows) for ref in xs], axis=0)
    for h in range(2):
        full = jnp.concatenate([c[...] for c in refs[h * steps : (h + 1) * steps]], axis=0)
        span = slice(h * cols, (h + 1) * cols)
        total = jnp.dot(x, full, preferred_element_type=F32)
        total = jnp.maximum(total * scale[:, span], 0.0)
        out[:, span] = (total * total).astype(BF16)


def up_project(order, scale, held, xs):
    steps = len(held)
    rows, width = xs[0].shape
    cols = held[0][0].shape[1]
    vmem = pl.BlockSpec(memory_space=pltpu.VMEM)
    return pl.pallas_call(
        functools.partial(up_kernel, steps, len(xs)),
        grid_spec=pltpu.PrefetchScalarGridSpec(
            num_scalar_prefetch=1,
            grid=(),
            in_specs=[vmem] * (1 + 2 * steps + len(xs)),
            out_specs=vmem,
        ),
        out_shape=jax.ShapeDtypeStruct((len(xs) * rows, 2 * cols), BF16),
        compiler_params=params(),
        cost_estimate=cost(
            4 * len(xs) * rows * width * cols,
            2 * (2 * width * cols + len(xs) * rows * (width + 2 * cols)),
        ),
        name="up_project",
    )(order, scale, *[h[0] for h in held], *[h[1] for h in held], *xs)


def down_kernel(steps, acts, *refs):
    a, chunks, outs = refs[:acts], refs[acts : acts + 2 * steps], refs[acts + 2 * steps :]
    half, cols = chunks[0].shape
    rows = outs[0].shape[1]
    for s in range(steps):
        for d, act in enumerate(a):
            total = jnp.dot(act[:, :half], chunks[2 * s][...], preferred_element_type=F32)
            total = total + jnp.dot(
                act[:, half:], chunks[2 * s + 1][...], preferred_element_type=F32
            )
            for i, out in enumerate(outs):
                out[d, :, s * cols : (s + 1) * cols] = total[i * rows : (i + 1) * rows].astype(
                    BF16
                )


def down_project(blocks, acts, held):
    rows, hidden = acts[0].shape
    rows = rows // blocks
    flat = [c for pair in held for c in pair]
    cols = flat[0].shape[1] * len(held)
    vmem = pl.BlockSpec(memory_space=pltpu.VMEM)
    return pl.pallas_call(
        functools.partial(down_kernel, len(held), len(acts)),
        in_specs=[vmem] * (len(acts) + len(flat)),
        out_specs=[vmem] * blocks,
        out_shape=[jax.ShapeDtypeStruct((len(acts), rows, cols), BF16)] * blocks,
        compiler_params=params(),
        cost_estimate=cost(
            2 * len(acts) * blocks * rows * hidden * cols,
            2 * (hidden * cols + len(acts) * blocks * rows * (hidden + cols)),
        ),
        name="down_project",
    )(*acts, *flat)


def sum_kernel(streams, count, order, *refs):
    total, squares = refs[-2:]
    where = []
    first = 0
    for groups in streams:
        where.append([(first + g, s) for g, steps in enumerate(groups) for s in range(steps)])
        first += len(groups)
    cols = total.shape[1] // count
    power = jnp.zeros(squares.shape, F32)
    for step in range(count - 1):
        value = None
        for places in where:
            g, s = places[step]
            part = refs[g][0, :, s * cols : (s + 1) * cols].astype(F32)
            value = part if value is None else value + part
        to = pl.multiple_of(order[step] * cols, cols)
        total[:, pl.ds(to, cols)] = value
        power = power + sum(
            value[:, at : at + LANES] * value[:, at : at + LANES] for at in range(0, cols, LANES)
        )
    to = pl.multiple_of(order[count - 1] * cols, cols)
    total[:, pl.ds(to, cols)] = jnp.zeros((total.shape[0], cols), F32)
    squares[...] = power


def sum_blocks(order, streams, parts, rows, width):
    tile = rows // 2
    flat = [p for stream in parts for p in stream]
    row = lambda n: pl.BlockSpec((tile, n), lambda i, *_: (i, 0))
    return pl.pallas_call(
        functools.partial(sum_kernel, streams, order.shape[0]),
        grid_spec=pltpu.PrefetchScalarGridSpec(
            num_scalar_prefetch=1,
            grid=(rows // tile,),
            in_specs=[
                pl.BlockSpec((1, tile, p.shape[2]), lambda i, *_: (0, i, 0)) for p in flat
            ],
            out_specs=[row(width), row(LANES)],
        ),
        out_shape=[
            jax.ShapeDtypeStruct((rows, width), F32),
            jax.ShapeDtypeStruct((rows, LANES), F32),
        ],
        compiler_params=params(),
        cost_estimate=cost(1e9, 2 * rows * width * (2 + len(streams))),
        name="sum_blocks",
    )(order, *flat)


def last_kernel(count, scalars, hidden, total, squares, *refs):
    ends, pieces = refs[: -2 - count], refs[-2 - count : -2]
    out, gains = refs[-2:]
    place_gains(scalars[count], pieces, gains)
    width = hidden.shape[1]
    cols = width // count
    end = ends[0][0].astype(F32)
    for ref in ends[1:]:
        end = end + ref[0].astype(F32)
    power = jnp.sum(squares[...], axis=-1, keepdims=True)
    power = power + jnp.sum(end * end, axis=-1, keepdims=True)
    scale = lax.rsqrt(power * (1.0 / width) + EPSILON)
    out[...] = (hidden[...].astype(F32) + total[...] * scale * gains[1:2, :]).astype(BF16)
    at = pl.ds(pl.multiple_of(scalars[count - 1] * cols, cols), cols)
    out[:, at] = (hidden[:, at].astype(F32) + end * scale * gains[1:2, at]).astype(BF16)


def last(scalars, hidden, total, squares, ends, gains):
    rows, width = hidden.shape
    tile = rows // 2
    row = lambda n: pl.BlockSpec((tile, n), lambda i, *_: (i, 0))
    part = lambda p: pl.BlockSpec((1, tile, p.shape[2]), lambda i, *_: (p.shape[0] - 1, i, 0))
    return pl.pallas_call(
        functools.partial(last_kernel, len(gains)),
        grid_spec=pltpu.PrefetchScalarGridSpec(
            num_scalar_prefetch=1,
            grid=(rows // tile,),
            in_specs=[row(width), row(width), row(LANES)]
            + [part(p) for p in ends]
            + [whole_spec(g.shape) for g in gains],
            out_specs=row(width),
            scratch_shapes=[pltpu.VMEM((2, width), F32)],
        ),
        out_shape=jax.ShapeDtypeStruct((rows, width), BF16),
        compiler_params=params(),
        cost_estimate=cost(1e9, 8 * rows * width),
        name="last",
    )(scalars, hidden, total, squares, *ends, *gains)


def group_sizes(count):
    far = (3,) + (2,) * (count // 2 - 2) + (1,) if count > 2 else (1, 1)
    return far, (count - 3, 2, 1)


def ring_device(
    reps,
    count,
    tps,
    tokens,
    gain_mix_pre,
    gain_mix_post,
    gain_mlp_pre,
    gain_mlp_post,
    x_weight,
    gate_weight,
    x_scale,
    gate_scale,
    conv_weight,
    recur_map,
    input_map,
    decay_param,
    out_weight,
    out_scale,
    up_weight,
    up_scale,
    down_weight,
    down_scale,
):
    rep, me, tp = (lax.axis_index(a) for a in ("rep", "fs", "tp"))
    length, width = tokens.shape[1:]
    share = length // tps
    chan = x_weight.shape[1] // reps
    hid = up_weight.shape[1] // reps

    def rep_part(value, size, axis):
        return lax.dynamic_slice_in_dim(value, rep * size, size, axis)

    rep_scalar, tp_scalar, me_scalar = (i.astype(jnp.int32).reshape(1) for i in (rep, tp, me))
    halves = prepare(
        rep_scalar, reps, x_weight, gate_weight, out_weight, gain_mix_pre[None], out_scale[None]
    )
    mixer = ring_gather(*halves, count)
    up_mine = (rep_part(up_weight, hid, 1) * gain_mlp_pre[:, None]).astype(BF16)
    ups = ring_gather(up_mine[:, : hid // 2], up_mine[:, hid // 2 :], count)
    down_mine = (rep_part(down_weight, hid, 0) * down_scale).astype(BF16)
    downs = ring_gather(down_mine[: hid // 2], down_mine[hid // 2 :], count)
    order = lax.dynamic_slice_in_dim(jnp.asarray(order_table(count)), me, 1, 0)[0]

    mine = lax.dynamic_slice_in_dim(tokens[0], tp * share, share, 0)
    seqs = [[tokens[0]]]
    for dr in range(1, reps):
        seqs.append([shift(mine, "rep", reps, dr)])
        for dt in range(1, tps):
            seqs[dr].append(shift(seqs[dr][0], "tp", tps, dt))
    normed_in = []
    for dr, pieces in enumerate(seqs):
        normed_in.append(normalize(tp_scalar if dr else 0 * tp_scalar, pieces))
    gains = exchange_small(jnp.stack([gain_mix_post, gain_mlp_post]), "fs", count)
    scales = jnp.concatenate([rep_part(x_scale, chan, 0), rep_part(gate_scale, chan, 0)])[None]
    same = jnp.asarray(
        (np.arange(LANES)[:, None] // BLOCK == np.arange(LANES)[None] // BLOCK), BF16
    )

    def dense_map(value):
        blocks = rep_part(value, chan, 0).reshape(chan // LANES, LANES, BLOCK)
        return jnp.tile(blocks, (1, 1, LANES // BLOCK)) * same

    maps = jnp.concatenate([dense_map(recur_map), dense_map(input_map)], axis=2)
    rate = -DECAY_SCALE * jax.nn.softplus(-rep_part(decay_param, chan, 0))[None]
    taps = rep_part(conv_weight, chan, 1)

    def over_tp(parts):
        got = [parts[0]]
        for dt in range(1, tps):
            got.append(shift(parts[dt], "tp", tps, tps - dt))
        return got

    def over_rep(summands, dr):
        total = sum(x.astype(F32) for x in summands).astype(BF16)
        return shift(total, "rep", reps, reps - dr)

    far_first = list(range(1, reps)) + [0]
    pieces = []
    for dr in far_first:
        x_branch, gate_branch = project(order, normed_in[dr], scales, mixer)
        mixed = recur(x_branch[None], gate_branch[None], taps, maps, rate)
        parts = out_project(order, tp_scalar, tps, mixed, mixer, width // count)
        summands = over_tp(parts)
        pieces += [over_rep(summands, dr)] if dr else summands
    hidden, normed = mid(me_scalar, mine, pieces, gains)

    scale = rep_part(up_scale, hid, 0)[None]
    acts = []
    for dr in range(reps):
        base = normed
        if dr:
            base = shift(normed, "rep", reps, dr)
        blocks = [base]
        for dt in range(1, tps):
            blocks.append(shift(base, "tp", tps, dt))
        acts.append(up_project(order, scale, ups, blocks))

    rows_of = {dr: [] for dr in far_first}
    for dr in far_first:
        groups = group_sizes(count)[0 if dr else 1]
        at = 0
        for steps in groups[:-1]:
            parts = down_project(tps, [acts[dr]], downs[at : at + steps])
            at += steps
            summands = over_tp(parts)
            rows_of[dr].append([over_rep(summands, dr)] if dr else summands)
    streams, arrays = [], []
    for dr in far_first:
        for i in range(len(rows_of[dr][0])):
            streams.append(group_sizes(count)[0 if dr else 1][:-1])
            arrays.append([group[i] for group in rows_of[dr]])
    total, squares = sum_blocks(order, tuple(streams), arrays, share, width)
    parts = down_project(tps, [acts[dr] for dr in far_first], downs[-1:])
    summands = over_tp(parts)
    ends = list(summands)
    for i, dr in enumerate(far_first):
        if dr:
            ends.append(over_rep([x[i : i + 1] for x in summands], dr))
    scalars = jnp.concatenate([order, me_scalar])
    return last(scalars, hidden, total, squares, ends, gains)[None]


def link_states(earlier, later):
    return (earlier[0] * later[0], later[0] * earlier[1] + later[1])


def plain_device(
    tokens,
    gain_mix_pre,
    gain_mix_post,
    gain_mlp_pre,
    gain_mlp_post,
    x_weight,
    gate_weight,
    x_scale,
    gate_scale,
    conv_weight,
    recur_map,
    input_map,
    decay_param,
    out_weight,
    out_scale,
    up_weight,
    up_scale,
    down_weight,
    down_scale,
):
    resid_in = tokens[0].astype(F32)
    length = resid_in.shape[0]
    local_width = x_weight.shape[1]
    gains = lax.all_gather(
        jnp.stack(
            [gain_mix_pre, gain_mix_post, gain_mlp_pre, gain_mlp_post, out_scale, down_scale]
        ),
        "fs",
        axis=1,
        tiled=True,
    )
    gather = lambda w, axis: lax.all_gather(w.astype(BF16), "fs", axis=axis, tiled=True)
    normed = rms_rows(resid_in, gains[0]).astype(BF16)
    x_proj = jnp.dot(normed, gather(x_weight, 0), preferred_element_type=F32)
    gate_proj = jnp.dot(normed, gather(gate_weight, 0), preferred_element_type=F32)
    out_cols = gather(out_weight, 1)
    down_full = gather(down_weight, 1)
    x_branch = (x_proj * x_scale).astype(BF16)
    gate_branch = (gate_proj * gate_scale).astype(BF16)
    taps = conv_weight.shape[0]
    padded = jnp.concatenate([jnp.zeros((taps - 1, local_width), BF16), x_branch], axis=0)
    conv_sum = conv_weight[0] * padded[0:length].astype(F32)
    for k in range(1, taps):
        conv_sum = conv_sum + conv_weight[k] * padded[k : k + length].astype(F32)
    conv_out = lax.optimization_barrier(conv_sum.astype(BF16))
    blocks = local_width // BLOCK
    conv_blocks = conv_out.reshape(length, blocks, BLOCK)

    def logits(value):
        return jnp.einsum(
            "tnc,ncd->tnd",
            conv_blocks,
            value.reshape(blocks, BLOCK, BLOCK),
            preferred_element_type=F32,
        ).reshape(length, local_width)

    log_decay = (
        -DECAY_SCALE * jax.nn.sigmoid(logits(recur_map)) * jax.nn.softplus(-decay_param)
    )
    drive = (
        jnp.sqrt(-jnp.expm1(2.0 * log_decay))
        * jax.nn.sigmoid(logits(input_map))
        * conv_out.astype(F32)
    )
    _, states = lax.associative_scan(link_states, (jnp.exp(log_decay), drive), axis=0)
    mixed = (states * jax.nn.gelu(gate_branch.astype(F32))).astype(BF16)
    share_rows = length // lax.axis_size("tp")

    def scatter(left, right, scale):
        part = (jnp.dot(left, right, preferred_element_type=F32) * scale).astype(BF16)
        return lax.psum_scatter(part, "tp", scatter_dimension=0, tiled=True).astype(F32)

    mix_share = scatter(mixed, out_cols, gains[4])
    resid_share = lax.dynamic_slice_in_dim(
        resid_in, lax.axis_index("tp") * share_rows, share_rows, 0
    )
    hidden_state = (resid_share + rms_rows(mix_share, gains[1])).astype(BF16)
    normed_mlp = rms_rows(hidden_state.astype(F32), gains[2]).astype(BF16)
    mlp_input = lax.all_gather(normed_mlp, "tp", axis=0, tiled=True)
    up_proj = jnp.dot(mlp_input, gather(up_weight, 0), preferred_element_type=F32)
    activated = jnp.square(jax.nn.relu(up_proj * up_scale)).astype(BF16)
    mlp_share = scatter(activated, down_full, gains[5])
    out_share = hidden_state.astype(F32) + rms_rows(mlp_share, gains[3])
    return out_share.astype(BF16)[None]


def solution(mesh):
    in_specs = (
        P(("rep", "fs"), None, None),
        P("fs"),
        P("fs"),
        P("fs"),
        P("fs"),
        P("fs", "tp"),
        P("fs", "tp"),
        P("tp"),
        P("tp"),
        P(None, "tp"),
        P("tp", None),
        P("tp", None),
        P("tp"),
        P("tp", "fs"),
        P("fs"),
        P("fs", "tp"),
        P("tp"),
        P("tp", "fs"),
        P("fs"),
    )
    reps, count, tps = (mesh.shape[a] for a in ("rep", "fs", "tp"))

    def on_device(*args):
        tokens, x_weight, up_weight = args[0], args[5], args[15]
        (length, width), rows = tokens.shape[1:], x_weight.shape[0]
        chan, hid = x_weight.shape[1] // reps, up_weight.shape[1] // reps
        fits = (
            count % 2 == 0
            and count >= 4
            and rows % (2 * LANES) == 0
            and chan % (2 * LANES) == 0
            and chan == 2 * rows
            and chan % (width // count) == 0
            and hid % (2 * LANES) == 0
            and length % (32 * tps) == 0
            and reps * (chan // LANES) <= 8
        )
        if fits:
            return ring_device(reps, count, tps, *args)
        return plain_device(*args)

    return jax.shard_map(
        on_device,
        mesh=mesh,
        in_specs=in_specs,
        out_specs=P(("rep", "fs"), "tp", None),
        check_vma=False,
    )
```

```python
import functools

import jax
import jax.numpy as jnp
import numpy as np
from jax import lax
from jax.experimental import pallas as pl
from jax.experimental.pallas import tpu as pltpu
from jax.sharding import PartitionSpec as P


BLOCK = 32
EPSILON = 1e-06
DECAY_SCALE = 8.0
BF16 = jnp.bfloat16
F32 = jnp.float32
LANES = 128
TIME_PAD = 8
VMEM_LIMIT = 24 * 1024 * 1024


def rms_rows(values, gain_vector):
    return (
        values
        * lax.rsqrt(jnp.mean(values * values, axis=-1, keepdims=True) + EPSILON)
        * gain_vector
    )


def params(limit=VMEM_LIMIT):
    return pltpu.CompilerParams(vmem_limit_bytes=limit)


def cost(flops, bytes_accessed, transcendentals=0):
    return pl.CostEstimate(
        flops=int(flops), bytes_accessed=int(bytes_accessed), transcendentals=int(transcendentals)
    )


def whole_spec(shape):
    zeros = (0,) * len(shape)
    return pl.BlockSpec(shape, lambda *_: zeros)


def ring_order(count):
    return list(range(0, count, 2)) + [i for i in range(count - 1, 0, -1) if i % 2]


def arrival(count):
    offsets = [0]
    for k in range(1, count // 2):
        offsets += [-k, k]
    return offsets + [count // 2]


def order_table(count):
    ring = ring_order(count)
    place = {dev: i for i, dev in enumerate(ring)}
    rows = [[ring[(place[m] + off) % count] for off in arrival(count)] for m in range(count)]
    return np.asarray(rows, np.int32)


def ring_gather(first, second, count, cuts=1):
    ring = ring_order(count)
    fwd = [(ring[i], ring[(i + 1) % count]) for i in range(count)]
    bwd = [(b, a) for a, b in fwd]
    far = count // 2
    ahead, behind = [first, second], [first, second]
    held = [(first, second)]
    for _ in range(1, far):
        for h in range(2):
            ahead[h] = lax.ppermute(ahead[h], "fs", fwd)
            behind[h] = lax.ppermute(behind[h], "fs", bwd)
        held += [tuple(ahead), tuple(behind)]
    for i in range(cuts):
        cols = slice(i * first.shape[1] // cuts, (i + 1) * first.shape[1] // cuts)
        one = lax.ppermute(ahead[0][:, cols], "fs", fwd)
        two = lax.ppermute(behind[1][:, cols], "fs", bwd)
        held.append((one, two))
    return held


def shift(value, axis, count, by):
    return lax.ppermute(value, axis, [((i + by) % count, i) for i in range(count)])


def exchange_small(value, axis, count):
    got = [value]
    for by in range(1, count):
        got.append(shift(value, axis, count, by))
    return got


def prepare_kernel(rep, x, gate, out, pre_all, scale_all, first, second, *scratch):
    x_own, gate_own, out_own, pre, scale, sems = scratch
    rows, cols = x_own.shape
    half = cols // 2
    wide = pl.ds(pl.multiple_of(rep[0] * cols, cols), cols)
    copies = [
        pltpu.make_async_copy(x.at[:, wide], x_own, sems.at[0]),
        pltpu.make_async_copy(gate.at[:, wide], gate_own, sems.at[1]),
        pltpu.make_async_copy(out.at[wide, :], out_own, sems.at[2]),
        pltpu.make_async_copy(pre_all, pre, sems.at[3]),
        pltpu.make_async_copy(scale_all, scale, sems.at[4]),
    ]
    for copy in copies:
        copy.start()
    copies[3].wait()
    gains = jnp.transpose(jnp.broadcast_to(pre[...], (LANES, rows)))
    for copy, own, to in ((copies[0], x_own, first), (copies[1], gate_own, second)):
        copy.wait()
        for at in range(0, cols, LANES):
            to[:, at : at + LANES] = (own[:, at : at + LANES] * gains).astype(BF16)
    copies[2].wait()
    copies[4].wait()
    first[:, cols:] = (out_own[:half, :] * scale[...]).astype(BF16)
    second[:, cols:] = (out_own[half:, :] * scale[...]).astype(BF16)


def prepare(rep, reps, x, gate, out, pre, scale):
    rows, cols = x.shape[0], x.shape[1] // reps
    shape = (rows, cols + out.shape[1])
    vmem = pl.BlockSpec(memory_space=pltpu.VMEM)
    hbm = pl.BlockSpec(memory_space=pltpu.HBM)
    return pl.pallas_call(
        prepare_kernel,
        grid_spec=pltpu.PrefetchScalarGridSpec(
            num_scalar_prefetch=1,
            grid=(),
            in_specs=[hbm] * 5,
            out_specs=[vmem] * 2,
            scratch_shapes=[
                pltpu.VMEM((rows, cols), F32),
                pltpu.VMEM((rows, cols), F32),
                pltpu.VMEM((cols, out.shape[1]), F32),
                pltpu.VMEM(pre.shape, F32),
                pltpu.VMEM(scale.shape, F32),
                pltpu.SemaphoreType.DMA((5,)),
            ],
        ),
        out_shape=[jax.ShapeDtypeStruct(shape, BF16)] * 2,
        compiler_params=params(62 * 1024 * 1024),
        cost_estimate=cost(1e6, 12 * rows * cols + 8 * rows * out.shape[1]),
        name="prepare",
    )(rep, x, gate, out, pre, scale)


def in_order(x, order, rows):
    steps = x.shape[1] // rows
    return jnp.concatenate(
        [x[:, pl.ds(pl.multiple_of(order[s] * rows, rows), rows)] for s in range(steps)], axis=1
    )


def norm_kernel(count, tp, *refs):
    out = refs[-1]
    for i in range(count):

        @pl.when(pl.program_id(0) == i)
        def _():
            v = refs[i][...].astype(F32)
            scale = lax.rsqrt(jnp.mean(v * v, axis=-1, keepdims=True) + EPSILON)
            out[...] = (v * scale).astype(BF16)


def normalize(tp, pieces):
    rows, width = pieces[0].shape
    count = len(pieces)
    return pl.pallas_call(
        functools.partial(norm_kernel, count),
        grid_spec=pltpu.PrefetchScalarGridSpec(
            num_scalar_prefetch=1,
            grid=(count,),
            in_specs=[whole_spec((rows, width))] * count,
            out_specs=pl.BlockSpec((rows, width), lambda i, tp: ((tp[0] + i) % count, 0)),
        ),
        out_shape=jax.ShapeDtypeStruct((count * rows, width), BF16),
        compiler_params=params(),
        cost_estimate=cost(1e9, 4 * count * rows * width),
        name="normalize",
    )(tp, *pieces)


def project_kernel(steps, order, normed, scale, *refs):
    outs = refs[2 * steps :]
    rows, cols = refs[0].shape[0], outs[0].shape[1]
    x = in_order(normed, order, rows)
    for h, out in enumerate(outs):
        full = jnp.concatenate([c[:, :cols] for c in refs[h * steps : (h + 1) * steps]], axis=0)
        total = jnp.dot(x, full, preferred_element_type=F32)
        out[...] = (total * scale[:, h * cols : (h + 1) * cols]).astype(BF16)


def project(order, normed, scale, held):
    steps = len(held)
    length, width = normed.shape
    cols = scale.shape[1] // 2
    out = jax.ShapeDtypeStruct((length, cols), BF16)
    vmem = pl.BlockSpec(memory_space=pltpu.VMEM)
    return pl.pallas_call(
        functools.partial(project_kernel, steps),
        grid_spec=pltpu.PrefetchScalarGridSpec(
            num_scalar_prefetch=1,
            grid=(),
            in_specs=[vmem] * (2 + 2 * steps),
            out_specs=[vmem, vmem],
        ),
        out_shape=[out, out],
        compiler_params=params(),
        cost_estimate=cost(4 * length * width * cols, 2 * (length + 2 * cols) * width),
        name="project",
    )(order, normed, scale, *[h[0] for h in held], *[h[1] for h in held])


def recur_kernel(x_ref, gate_ref, conv_ref, maps_ref, rate_ref, out_ref, pad, decay, state):
    seqs, length, width = x_ref.shape
    blocks = width // LANES
    lines = seqs * blocks
    stride = length + TIME_PAD
    taps = conv_ref.shape[0]
    pad[0:TIME_PAD, :] = jnp.zeros((TIME_PAD, LANES), F32)
    for q in range(seqs):
        for b in range(blocks):
            cols = slice(b * LANES, (b + 1) * LANES)
            base = (q * blocks + b) * stride
            pad[TIME_PAD:, :] = x_ref[q, :, cols].astype(F32)
            total = None
            for k in range(taps):
                at = TIME_PAD - (taps - 1) + k
                part = conv_ref[k : k + 1, cols] * pad[at : at + length, :]
                total = part if total is None else total + part
            conv = total.astype(BF16)
            logits = jnp.dot(conv, maps_ref[b], preferred_element_type=F32)
            log_decay = rate_ref[:, cols] * jax.nn.sigmoid(logits[:, :LANES])
            a = jnp.exp(log_decay)
            y = 2.0 * log_decay
            series = -y * (
                1.0
                + y * (1 / 2 + y * (1 / 6 + y * (1 / 24 + y * (1 / 120 + y * (1 / 720)))))
            )
            loss = jnp.where(y > -0.4, series, 1.0 - a * a)
            decay[base : base + length, :] = a
            state[base : base + length, :] = (
                jnp.sqrt(loss) * jax.nn.sigmoid(logits[:, LANES:]) * conv.astype(F32)
            )

    def advance(t, h):
        at = pl.ds(t, lines, stride=stride)
        h = decay[at, :] * h + state[at, :]
        state[at, :] = h
        return h

    lax.fori_loop(0, length, advance, jnp.zeros((lines, LANES), F32), unroll=16)
    for q in range(seqs):
        for b in range(blocks):
            cols = slice(b * LANES, (b + 1) * LANES)
            base = (q * blocks + b) * stride
            g = gate_ref[q, :, cols].astype(F32)
            out_ref[q, :, cols] = (
                state[base : base + length, :] * jax.nn.gelu(g)
            ).astype(BF16)


def recur(x_branch, gate_branch, conv_weight, maps, rate):
    seqs, length, width = x_branch.shape
    lines = seqs * (width // LANES)
    rows = lines * (length + TIME_PAD)
    vmem = pl.BlockSpec(memory_space=pltpu.VMEM)
    return pl.pallas_call(
        recur_kernel,
        in_specs=[vmem] * 5,
        out_specs=vmem,
        out_shape=jax.ShapeDtypeStruct(x_branch.shape, BF16),
        scratch_shapes=[
            pltpu.VMEM((length + TIME_PAD, LANES), F32),
            pltpu.VMEM((rows, LANES), F32),
            pltpu.VMEM((rows, LANES), F32),
        ],
        compiler_params=params(),
        cost_estimate=cost(3e9, 6 * x_branch.size, 10 * x_branch.size),
        name="recur",
    )(x_branch, gate_branch, conv_weight, maps, rate)


def out_kernel(steps, cols, order, mixed, *refs):
    top, low = refs[:steps], refs[steps : 2 * steps]
    outs = refs[2 * steps :]
    tps, share = len(outs), outs[0].shape[1]
    half = top[0].shape[0]
    pieces = []
    for j in range(tps):
        at = pl.multiple_of((order[steps] + j) % tps * share, share)
        pieces.append(mixed[0, pl.ds(at, share), :])
    m = jnp.concatenate(pieces, axis=0)
    for s in range(steps):
        at = pl.multiple_of(order[s] * cols, cols)
        part = jnp.dot(m[:, :half], top[s][:, -cols:], preferred_element_type=F32)
        part = part + jnp.dot(m[:, half:], low[s][:, -cols:], preferred_element_type=F32)
        for j, out in enumerate(outs):
            out[0, :, pl.ds(at, cols)] = part[j * share : (j + 1) * share].astype(BF16)


def out_project(order, tp, tps, mixed, held, cols):
    steps = len(held)
    _, length, width = mixed.shape
    share = length // tps
    scalars = jnp.concatenate([order, tp])
    vmem = pl.BlockSpec(memory_space=pltpu.VMEM)
    return pl.pallas_call(
        functools.partial(out_kernel, steps, cols),
        grid_spec=pltpu.PrefetchScalarGridSpec(
            num_scalar_prefetch=1,
            grid=(),
            in_specs=[vmem] * (1 + 2 * steps),
            out_specs=[vmem] * tps,
        ),
        out_shape=[jax.ShapeDtypeStruct((1, share, steps * cols), BF16)] * tps,
        compiler_params=params(),
        cost_estimate=cost(
            2 * length * width * steps * cols,
            2 * (width * steps * cols + length * (width + steps * cols)),
        ),
        name="out_project",
    )(scalars, mixed, *[h[0] for h in held], *[h[1] for h in held])


def place_gains(me, pieces, gains):
    count, cols = len(pieces), pieces[0].shape[1]
    for i, piece in enumerate(pieces):
        at = pl.multiple_of((me + i) % count * cols, cols)
        gains[:, pl.ds(at, cols)] = piece[...]


def mid_kernel(count, me, tokens, *refs):
    parts, pieces = refs[: -3 - count], refs[-3 - count : -3]
    hidden, normed, gains = refs[-3:]
    place_gains(me[0], pieces, gains)
    total = parts[0][0].astype(F32)
    for part in parts[1:]:
        total = total + part[0].astype(F32)
    h = (
        tokens[...].astype(F32)
        + total
        * lax.rsqrt(jnp.mean(total * total, axis=-1, keepdims=True) + EPSILON)
        * gains[0:1, :]
    ).astype(BF16)
    hidden[...] = h
    v = h.astype(F32)
    normed[...] = (
        v * lax.rsqrt(jnp.mean(v * v, axis=-1, keepdims=True) + EPSILON)
    ).astype(BF16)


def mid(me, tokens, parts, gains):
    rows, width = tokens.shape
    tile = rows // 2
    row = pl.BlockSpec((tile, width), lambda i, *_: (i, 0))
    part = pl.BlockSpec((1, tile, width), lambda i, *_: (0, i, 0))
    out = jax.ShapeDtypeStruct((rows, width), BF16)
    return pl.pallas_call(
        functools.partial(mid_kernel, len(gains)),
        grid_spec=pltpu.PrefetchScalarGridSpec(
            num_scalar_prefetch=1,
            grid=(rows // tile,),
            in_specs=[row] + [part] * len(parts) + [whole_spec(g.shape) for g in gains],
            out_specs=[row, row],
            scratch_shapes=[pltpu.VMEM((2, width), F32)],
        ),
        out_shape=[out, out],
        compiler_params=params(),
        cost_estimate=cost(2e9, 2 * rows * width * (3 + len(parts))),
        name="mid",
    )(me, tokens, *parts, *gains)


def up_kernel(steps, blocks, order, scale, *refs):
    xs = refs[2 * steps : 2 * steps + blocks]
    out = refs[-1]
    rows, cols = refs[0].shape
    x = jnp.concatenate([in_order(ref, order, rows) for ref in xs], axis=0)
    for h in range(2):
        full = jnp.concatenate([c[...] for c in refs[h * steps : (h + 1) * steps]], axis=0)
        span = slice(h * cols, (h + 1) * cols)
        total = jnp.dot(x, full, preferred_element_type=F32)
        total = jnp.maximum(total * scale[:, span], 0.0)
        out[:, span] = (total * total).astype(BF16)


def up_project(order, scale, held, xs):
    steps = len(held)
    rows, width = xs[0].shape
    cols = held[0][0].shape[1]
    vmem = pl.BlockSpec(memory_space=pltpu.VMEM)
    return pl.pallas_call(
        functools.partial(up_kernel, steps, len(xs)),
        grid_spec=pltpu.PrefetchScalarGridSpec(
            num_scalar_prefetch=1,
            grid=(),
            in_specs=[vmem] * (1 + 2 * steps + len(xs)),
            out_specs=vmem,
        ),
        out_shape=jax.ShapeDtypeStruct((len(xs) * rows, 2 * cols), BF16),
        compiler_params=params(),
        cost_estimate=cost(
            4 * len(xs) * rows * width * cols,
            2 * (2 * width * cols + len(xs) * rows * (width + 2 * cols)),
        ),
        name="up_project",
    )(order, scale, *[h[0] for h in held], *[h[1] for h in held], *xs)


def down_kernel(steps, acts, *refs):
    a, chunks, outs = refs[:acts], refs[acts : acts + 2 * steps], refs[acts + 2 * steps :]
    half, cols = chunks[0].shape
    rows = outs[0].shape[1]
    for s in range(steps):
        for d, act in enumerate(a):
            total = jnp.dot(act[:, :half], chunks[2 * s][...], preferred_element_type=F32)
            total = total + jnp.dot(
                act[:, half:], chunks[2 * s + 1][...], preferred_element_type=F32
            )
            for i, out in enumerate(outs):
                out[d, :, s * cols : (s + 1) * cols] = total[i * rows : (i + 1) * rows].astype(
                    BF16
                )


def down_project(blocks, acts, held):
    rows, hidden = acts[0].shape
    rows = rows // blocks
    flat = [c for pair in held for c in pair]
    cols = flat[0].shape[1] * len(held)
    vmem = pl.BlockSpec(memory_space=pltpu.VMEM)
    return pl.pallas_call(
        functools.partial(down_kernel, len(held), len(acts)),
        in_specs=[vmem] * (len(acts) + len(flat)),
        out_specs=[vmem] * blocks,
        out_shape=[jax.ShapeDtypeStruct((len(acts), rows, cols), BF16)] * blocks,
        compiler_params=params(),
        cost_estimate=cost(
            2 * len(acts) * blocks * rows * hidden * cols,
            2 * (hidden * cols + len(acts) * blocks * rows * (hidden + cols)),
        ),
        name="down_project",
    )(*acts, *flat)


def sum_kernel(streams, count, order, *refs):
    total, squares = refs[-2:]
    where = []
    first = 0
    for groups in streams:
        where.append([(first + g, s) for g, steps in enumerate(groups) for s in range(steps)])
        first += len(groups)
    cols = total.shape[1] // count
    power = jnp.zeros(squares.shape, F32)
    for step in range(count - 1):
        value = None
        for places in where:
            g, s = places[step]
            part = refs[g][0, :, s * cols : (s + 1) * cols].astype(F32)
            value = part if value is None else value + part
        to = pl.multiple_of(order[step] * cols, cols)
        total[:, pl.ds(to, cols)] = value
        power = power + sum(
            value[:, at : at + LANES] * value[:, at : at + LANES] for at in range(0, cols, LANES)
        )
    to = pl.multiple_of(order[count - 1] * cols, cols)
    total[:, pl.ds(to, cols)] = jnp.zeros((total.shape[0], cols), F32)
    squares[...] = power


def sum_blocks(order, streams, parts, rows, width):
    tile = rows // 2
    flat = [p for stream in parts for p in stream]
    row = lambda n: pl.BlockSpec((tile, n), lambda i, *_: (i, 0))
    return pl.pallas_call(
        functools.partial(sum_kernel, streams, order.shape[0]),
        grid_spec=pltpu.PrefetchScalarGridSpec(
            num_scalar_prefetch=1,
            grid=(rows // tile,),
            in_specs=[
                pl.BlockSpec((1, tile, p.shape[2]), lambda i, *_: (0, i, 0)) for p in flat
            ],
            out_specs=[row(width), row(LANES)],
        ),
        out_shape=[
            jax.ShapeDtypeStruct((rows, width), F32),
            jax.ShapeDtypeStruct((rows, LANES), F32),
        ],
        compiler_params=params(),
        cost_estimate=cost(1e9, 2 * rows * width * (2 + len(streams))),
        name="sum_blocks",
    )(order, *flat)


def last_kernel(count, cuts, scalars, hidden, total, squares, *refs):
    ends, pieces = refs[: -2 - count], refs[-2 - count : -2]
    out, gains = refs[-2:]
    place_gains(scalars[count], pieces, gains)
    width = hidden.shape[1]
    cols = width // count // cuts
    each = len(ends) // cuts
    power = jnp.sum(squares[...], axis=-1, keepdims=True)
    sums = []
    for i in range(cuts):
        end = ends[i * each][0].astype(F32)
        for ref in ends[i * each + 1 : (i + 1) * each]:
            end = end + ref[0].astype(F32)
        sums.append(end)
        power = power + jnp.sum(end * end, axis=-1, keepdims=True)
    scale = lax.rsqrt(power * (1.0 / width) + EPSILON)
    out[...] = (hidden[...].astype(F32) + total[...] * scale * gains[1:2, :]).astype(BF16)
    for i, end in enumerate(sums):
        at = pl.ds(pl.multiple_of((scalars[count - 1] * cuts + i) * cols, cols), cols)
        out[:, at] = (hidden[:, at].astype(F32) + end * scale * gains[1:2, at]).astype(BF16)


def last(scalars, hidden, total, squares, ends, gains, cuts):
    rows, width = hidden.shape
    tile = rows // 2
    row = lambda n: pl.BlockSpec((tile, n), lambda i, *_: (i, 0))
    part = lambda p: pl.BlockSpec((1, tile, p.shape[2]), lambda i, *_: (p.shape[0] - 1, i, 0))
    return pl.pallas_call(
        functools.partial(last_kernel, len(gains), cuts),
        grid_spec=pltpu.PrefetchScalarGridSpec(
            num_scalar_prefetch=1,
            grid=(rows // tile,),
            in_specs=[row(width), row(width), row(LANES)]
            + [part(p) for p in ends]
            + [whole_spec(g.shape) for g in gains],
            out_specs=row(width),
            scratch_shapes=[pltpu.VMEM((2, width), F32)],
        ),
        out_shape=jax.ShapeDtypeStruct((rows, width), BF16),
        compiler_params=params(),
        cost_estimate=cost(1e9, 8 * rows * width),
        name="last",
    )(scalars, hidden, total, squares, *ends, *gains)


FAR_CUTS = 2


def group_sizes(count):
    far = (3,) + (2,) * (count // 2 - 2) + (1,) if count > 2 else (1, 1)
    return far, (count - 3, 2, 1)


def ring_device(
    reps,
    count,
    tps,
    tokens,
    gain_mix_pre,
    gain_mix_post,
    gain_mlp_pre,
    gain_mlp_post,
    x_weight,
    gate_weight,
    x_scale,
    gate_scale,
    conv_weight,
    recur_map,
    input_map,
    decay_param,
    out_weight,
    out_scale,
    up_weight,
    up_scale,
    down_weight,
    down_scale,
):
    rep, me, tp = (lax.axis_index(a) for a in ("rep", "fs", "tp"))
    length, width = tokens.shape[1:]
    share = length // tps
    chan = x_weight.shape[1] // reps
    hid = up_weight.shape[1] // reps

    def rep_part(value, size, axis):
        return lax.dynamic_slice_in_dim(value, rep * size, size, axis)

    rep_scalar, tp_scalar, me_scalar = (i.astype(jnp.int32).reshape(1) for i in (rep, tp, me))
    halves = prepare(
        rep_scalar, reps, x_weight, gate_weight, out_weight, gain_mix_pre[None], out_scale[None]
    )
    mixer = ring_gather(*halves, count)
    up_mine = (rep_part(up_weight, hid, 1) * gain_mlp_pre[:, None]).astype(BF16)
    ups = ring_gather(up_mine[:, : hid // 2], up_mine[:, hid // 2 :], count)
    down_mine = (rep_part(down_weight, hid, 0) * down_scale).astype(BF16)
    downs = ring_gather(down_mine[: hid // 2], down_mine[hid // 2 :], count, FAR_CUTS)
    order = lax.dynamic_slice_in_dim(jnp.asarray(order_table(count)), me, 1, 0)[0]

    mine = lax.dynamic_slice_in_dim(tokens[0], tp * share, share, 0)
    seqs = [[tokens[0]]]
    for dr in range(1, reps):
        seqs.append([shift(mine, "rep", reps, dr)])
        for dt in range(1, tps):
            seqs[dr].append(shift(seqs[dr][0], "tp", tps, dt))
    normed_in = []
    for dr, pieces in enumerate(seqs):
        normed_in.append(normalize(tp_scalar if dr else 0 * tp_scalar, pieces))
    gains = exchange_small(jnp.stack([gain_mix_post, gain_mlp_post]), "fs", count)
    scales = jnp.concatenate([rep_part(x_scale, chan, 0), rep_part(gate_scale, chan, 0)])[None]
    same = jnp.asarray(
        (np.arange(LANES)[:, None] // BLOCK == np.arange(LANES)[None] // BLOCK), BF16
    )

    def dense_map(value):
        blocks = rep_part(value, chan, 0).reshape(chan // LANES, LANES, BLOCK)
        return jnp.tile(blocks, (1, 1, LANES // BLOCK)) * same

    maps = jnp.concatenate([dense_map(recur_map), dense_map(input_map)], axis=2)
    rate = -DECAY_SCALE * jax.nn.softplus(-rep_part(decay_param, chan, 0))[None]
    taps = rep_part(conv_weight, chan, 1)

    def over_tp(parts):
        got = [parts[0]]
        for dt in range(1, tps):
            got.append(shift(parts[dt], "tp", tps, tps - dt))
        return got

    def over_rep(summands, dr):
        total = sum(x.astype(F32) for x in summands).astype(BF16)
        return shift(total, "rep", reps, reps - dr)

    far_first = list(range(1, reps)) + [0]
    pieces = []
    for dr in far_first:
        x_branch, gate_branch = project(order, normed_in[dr], scales, mixer)
        mixed = recur(x_branch[None], gate_branch[None], taps, maps, rate)
        parts = out_project(order, tp_scalar, tps, mixed, mixer, width // count)
        summands = over_tp(parts)
        pieces += [over_rep(summands, dr)] if dr else summands
    hidden, normed = mid(me_scalar, mine, pieces, gains)

    scale = rep_part(up_scale, hid, 0)[None]
    acts = []
    for dr in range(reps):
        base = normed
        if dr:
            base = shift(normed, "rep", reps, dr)
        blocks = [base]
        for dt in range(1, tps):
            blocks.append(shift(base, "tp", tps, dt))
        acts.append(up_project(order, scale, ups, blocks))

    rows_of = {dr: [] for dr in far_first}
    for dr in far_first:
        groups = group_sizes(count)[0 if dr else 1]
        at = 0
        for steps in groups[:-1]:
            parts = down_project(tps, [acts[dr]], downs[at : at + steps])
            at += steps
            summands = over_tp(parts)
            rows_of[dr].append([over_rep(summands, dr)] if dr else summands)
    streams, arrays = [], []
    for dr in far_first:
        for i in range(len(rows_of[dr][0])):
            streams.append(group_sizes(count)[0 if dr else 1][:-1])
            arrays.append([group[i] for group in rows_of[dr]])
    total, squares = sum_blocks(order, tuple(streams), arrays, share, width)
    ends = []
    for cut in range(FAR_CUTS):
        parts = down_project(
            tps, [acts[dr] for dr in far_first], downs[count - 1 + cut : count + cut]
        )
        summands = over_tp(parts)
        ends += summands
        for i, dr in enumerate(far_first):
            if dr:
                ends.append(over_rep([x[i : i + 1] for x in summands], dr))
    scalars = jnp.concatenate([order, me_scalar])
    return last(scalars, hidden, total, squares, ends, gains, FAR_CUTS)[None]


def link_states(earlier, later):
    return (earlier[0] * later[0], later[0] * earlier[1] + later[1])


def plain_device(
    tokens,
    gain_mix_pre,
    gain_mix_post,
    gain_mlp_pre,
    gain_mlp_post,
    x_weight,
    gate_weight,
    x_scale,
    gate_scale,
    conv_weight,
    recur_map,
    input_map,
    decay_param,
    out_weight,
    out_scale,
    up_weight,
    up_scale,
    down_weight,
    down_scale,
):
    resid_in = tokens[0].astype(F32)
    length = resid_in.shape[0]
    local_width = x_weight.shape[1]
    gains = lax.all_gather(
        jnp.stack(
            [gain_mix_pre, gain_mix_post, gain_mlp_pre, gain_mlp_post, out_scale, down_scale]
        ),
        "fs",
        axis=1,
        tiled=True,
    )
    gather = lambda w, axis: lax.all_gather(w.astype(BF16), "fs", axis=axis, tiled=True)
    normed = rms_rows(resid_in, gains[0]).astype(BF16)
    x_proj = jnp.dot(normed, gather(x_weight, 0), preferred_element_type=F32)
    gate_proj = jnp.dot(normed, gather(gate_weight, 0), preferred_element_type=F32)
    out_cols = gather(out_weight, 1)
    down_full = gather(down_weight, 1)
    x_branch = (x_proj * x_scale).astype(BF16)
    gate_branch = (gate_proj * gate_scale).astype(BF16)
    taps = conv_weight.shape[0]
    padded = jnp.concatenate([jnp.zeros((taps - 1, local_width), BF16), x_branch], axis=0)
    conv_sum = conv_weight[0] * padded[0:length].astype(F32)
    for k in range(1, taps):
        conv_sum = conv_sum + conv_weight[k] * padded[k : k + length].astype(F32)
    conv_out = lax.optimization_barrier(conv_sum.astype(BF16))
    blocks = local_width // BLOCK
    conv_blocks = conv_out.reshape(length, blocks, BLOCK)

    def logits(value):
        return jnp.einsum(
            "tnc,ncd->tnd",
            conv_blocks,
            value.reshape(blocks, BLOCK, BLOCK),
            preferred_element_type=F32,
        ).reshape(length, local_width)

    log_decay = (
        -DECAY_SCALE * jax.nn.sigmoid(logits(recur_map)) * jax.nn.softplus(-decay_param)
    )
    drive = (
        jnp.sqrt(-jnp.expm1(2.0 * log_decay))
        * jax.nn.sigmoid(logits(input_map))
        * conv_out.astype(F32)
    )
    _, states = lax.associative_scan(link_states, (jnp.exp(log_decay), drive), axis=0)
    mixed = (states * jax.nn.gelu(gate_branch.astype(F32))).astype(BF16)
    share_rows = length // lax.axis_size("tp")

    def scatter(left, right, scale):
        part = (jnp.dot(left, right, preferred_element_type=F32) * scale).astype(BF16)
        return lax.psum_scatter(part, "tp", scatter_dimension=0, tiled=True).astype(F32)

    mix_share = scatter(mixed, out_cols, gains[4])
    resid_share = lax.dynamic_slice_in_dim(
        resid_in, lax.axis_index("tp") * share_rows, share_rows, 0
    )
    hidden_state = (resid_share + rms_rows(mix_share, gains[1])).astype(BF16)
    normed_mlp = rms_rows(hidden_state.astype(F32), gains[2]).astype(BF16)
    mlp_input = lax.all_gather(normed_mlp, "tp", axis=0, tiled=True)
    up_proj = jnp.dot(mlp_input, gather(up_weight, 0), preferred_element_type=F32)
    activated = jnp.square(jax.nn.relu(up_proj * up_scale)).astype(BF16)
    mlp_share = scatter(activated, down_full, gains[5])
    out_share = hidden_state.astype(F32) + rms_rows(mlp_share, gains[3])
    return out_share.astype(BF16)[None]


def solution(mesh):
    in_specs = (
        P(("rep", "fs"), None, None),
        P("fs"),
        P("fs"),
        P("fs"),
        P("fs"),
        P("fs", "tp"),
        P("fs", "tp"),
        P("tp"),
        P("tp"),
        P(None, "tp"),
        P("tp", None),
        P("tp", None),
        P("tp"),
        P("tp", "fs"),
        P("fs"),
        P("fs", "tp"),
        P("tp"),
        P("tp", "fs"),
        P("fs"),
    )
    reps, count, tps = (mesh.shape[a] for a in ("rep", "fs", "tp"))

    def on_device(*args):
        tokens, x_weight, up_weight = args[0], args[5], args[15]
        (length, width), rows = tokens.shape[1:], x_weight.shape[0]
        chan, hid = x_weight.shape[1] // reps, up_weight.shape[1] // reps
        fits = (
            count % 2 == 0
            and count >= 4
            and rows % (2 * LANES) == 0
            and chan % (2 * LANES) == 0
            and chan == 2 * rows
            and chan % (width // count) == 0
            and hid % (2 * LANES) == 0
            and width // count % (FAR_CUTS * LANES) == 0
            and length % (32 * tps) == 0
            and reps * (chan // LANES) <= 8
        )
        if fits:
            return ring_device(reps, count, tps, *args)
        return plain_device(*args)

    return jax.shard_map(
        on_device,
        mesh=mesh,
        in_specs=in_specs,
        out_specs=P(("rep", "fs"), "tp", None),
        check_vma=False,
    )
```
